512 devices in a mesh: sp: 64 (over z, y), tp: 8 (over x, core).
Axes of the slice: x: 4, y: 4, z: 16, core: 2. Of those that a mesh axis runs over, the one named last changes fastest.
Arguments:
- prompt: bfloat16 [8, 4096, 2048], P(None, 'sp'), may hold values from -6 to 6
- keep_scale: float32 [8, 4096], P(None, 'sp'), may hold values from 0.25 to 1
- new_token: bfloat16 [8, 2048], P(None, 'tp'), may hold values from -6 to 6
- w_query: bfloat16 [2048, 1024], P(None, 'tp'), may hold values from -0.125 to 0.125
- w_forget: bfloat16 [2048, 1024], P(None, 'tp'), may hold values from -0.125 to 0.125
- w_value: bfloat16 [2048, 1024], P(None, 'tp'), may hold values from -4.21875 to 4.21875
- w_outgate: bfloat16 [2048, 1024], P(None, 'tp'), may hold values from -0.125 to 0.125
- floor_gap: float32 [1024], P('tp'), may hold values from 0 to 0.06
- norm_gain: float32 [128], replicated, may hold values from 0.1 to 1.9
Outputs:
- state_cache: bfloat16 [8, 1024, 128], P('tp', 'sp')
- first_read: bfloat16 [8, 1024], P(None, 'tp')
The draws below stay inside these ranges and needn't reach their ends.
All inputs are finite; a program needn't handle non-finite values.
Results may differ from the reference program's by a relative error of at most 0.0022.
The reference program's roundings to bfloat16 on the way (of `values` and `new_value`) count: a program that leaves them out, or rounds other values in their place, can miss the bound.
Values may be sent and summed in bfloat16 or wider, within the bound.
No kernel may reach another device: no remote copies, remote signals or barrier semaphores. Data moves between devices by JAX's collectives and lax.ppermute only.
A program may use at most 64 MiB of HBM per device.

```python
import math
import jax
import jax.numpy as jnp
from jax import lax

D = 2048
HEADS = 8
HEAD_DIM = 128
MIX_WIDTH = 1024
PROMPT_COUNT = 8
TOK_SEQ = 64
PROMPT_LENGTH = 4096


def draw_keep_scale(key, part):
    key_rate = jax.random.fold_in(key, 11)
    key_positions = jax.random.fold_in(key, 12)
    key_depth = jax.random.fold_in(key, 13)
    blocks = PROMPT_LENGTH // TOK_SEQ
    block_rate = jnp.exp(jax.random.uniform(key_rate, (PROMPT_COUNT, blocks, 1), minval=math.log(0.4), maxval=math.log(1.6))) / PROMPT_LENGTH
    steady = jnp.broadcast_to(jnp.exp(-block_rate), (PROMPT_COUNT, blocks, TOK_SEQ)).reshape(PROMPT_COUNT, PROMPT_LENGTH)
    spike_positions = jax.random.randint(key_positions, (PROMPT_COUNT, 2), 0, PROMPT_LENGTH)
    spike_match = jnp.arange(PROMPT_LENGTH, dtype=jnp.int32)[None, None, :] == spike_positions[:, :, None]
    intensity = jax.random.uniform(key_depth, (PROMPT_COUNT, 2, 1), minval=0.55, maxval=0.8)
    multiplier = jnp.prod(jnp.where(spike_match, intensity, 1.0), axis=1)
    return (steady * multiplier).astype(jnp.float32)


def draw_floor_gap(key, part):
    key_order = jax.random.fold_in(key, 21)
    key_fast = jax.random.fold_in(key, 22)
    key_slow = jax.random.fold_in(key, 23)
    head_order = jax.random.permutation(key_order, HEADS)
    fast_count = HEADS // 2
    fast_head = head_order < fast_count
    fast_gap = jnp.exp(jax.random.uniform(key_fast, (HEADS, HEAD_DIM), minval=math.log(0.02), maxval=math.log(0.06)))
    slow_gap = jnp.exp(jax.random.uniform(key_slow, (HEADS, HEAD_DIM), minval=math.log(0.2), maxval=0.0)) / PROMPT_LENGTH
    return jnp.where(fast_head[:, None], fast_gap, slow_gap).reshape(HEADS * HEAD_DIM).astype(jnp.float32)


def levels(key, extent, split, least, largest):
    factor_of = 1.0
    for position, parts in split:
        steps = jax.random.uniform(jax.random.fold_in(jax.random.fold_in(key, 6), position), (parts,), jnp.float32, least / len(split), largest / len(split))
        factor_of = factor_of * jnp.repeat(jnp.exp(steps), extent[position] // parts).reshape((-1,) + (1,) * (len(extent) - 1 - position))
    return factor_of


def normal_values(key, dims, deviation, most, split=(), kind=jnp.bfloat16):
    values = jax.random.normal(key, dims, jnp.float32) * deviation
    if len(split) > 0:
        values = levels(key, dims, split, -0.22, 0.18) * values
    return jnp.clip(values, min=-most, max=most).astype(kind)


def setup_inputs(seed: int = 0) -> dict:
    splits = jax.random.split(jax.random.key(seed), 10)
    return {
        "prompt": normal_values(splits[0], (PROMPT_COUNT, PROMPT_LENGTH, D), 1.0, 6.0, ((1, 64),)),
        "keep_scale": draw_keep_scale(jax.random.fold_in(splits[9], 71), 0),
        "new_token": normal_values(splits[2], (PROMPT_COUNT, D), 1.0, 6.0, ((1, 8),)),
        "w_query": normal_values(splits[3], (D, MIX_WIDTH), D ** -0.5, 0.125, ((1, 8),)),
        "w_forget": normal_values(splits[4], (D, MIX_WIDTH), D ** -0.5, 0.125, ((1, 8),)),
        "w_value": normal_values(splits[5], (D, MIX_WIDTH), (0.5 * PROMPT_LENGTH ** 0.5 * D ** -0.5), 4.21875, ((1, 8),)),
        "w_outgate": normal_values(splits[6], (D, MIX_WIDTH), D ** -0.5, 0.125, ((1, 8),)),
        "floor_gap": draw_floor_gap(jax.random.fold_in(splits[9], 71), 0),
        "norm_gain": jnp.clip(1.0 + 0.18 * jax.random.normal(splits[8], (HEAD_DIM,), jnp.float32), 0.1, 1.9),
    }


EPSILON = 1e-06

def reference(prompt, keep_scale, new_token, w_query, w_forget, w_value, w_outgate, floor_gap, norm_gain):
    floor_rows = floor_gap.reshape(HEADS, HEAD_DIM)

    def one_sequence(inputs):
        seq_rows, keep_row = inputs
        forget_pre = jnp.dot(seq_rows, w_forget, preferred_element_type=jnp.float32).reshape(PROMPT_LENGTH, HEADS, HEAD_DIM)
        values = jnp.dot(seq_rows, w_value, preferred_element_type=jnp.float32).astype(jnp.bfloat16)
        values = lax.optimization_barrier(values).astype(jnp.float32).reshape(PROMPT_LENGTH, HEADS, HEAD_DIM)
        forget_loss = floor_rows * (1.0 - jax.nn.sigmoid(forget_pre))
        keep_factor = keep_row[:, None, None]
        log_forget = jnp.log(keep_factor) + jnp.log1p(-forget_loss)
        input_gate = 1.0 - keep_factor + keep_factor * forget_loss
        later_log = lax.cumsum(log_forget, axis=0, reverse=True) - log_forget
        return jnp.einsum('thc,thv->hcv', input_gate * jnp.exp(later_log), values, precision=lax.Precision.HIGHEST)
    final_state = lax.map(one_sequence, (prompt, keep_scale))
    state_cache = final_state.transpose(1, 0, 2, 3).reshape(HEADS, PROMPT_COUNT * HEAD_DIM, HEAD_DIM).astype(jnp.bfloat16)
    shaped = (PROMPT_COUNT, HEADS, HEAD_DIM)
    query = jnp.dot(new_token, w_query, preferred_element_type=jnp.float32).reshape(shaped)
    new_forget = jnp.dot(new_token, w_forget, preferred_element_type=jnp.float32).reshape(shaped)
    new_gate = jnp.dot(new_token, w_outgate, preferred_element_type=jnp.float32).reshape(shaped)
    new_value = jnp.dot(new_token, w_value, preferred_element_type=jnp.float32).astype(jnp.bfloat16)
    new_value = lax.optimization_barrier(new_value).astype(jnp.float32).reshape(shaped)
    new_loss = floor_rows * (1.0 - jax.nn.sigmoid(new_forget))
    mixed = jnp.einsum('shc,shcv->shv', query * (1.0 - new_loss), final_state, precision=lax.Precision.HIGHEST)
    mixed = mixed + lax.optimization_barrier(jnp.sum(query * new_loss, axis=-1, keepdims=True)) * new_value
    normed = mixed * lax.rsqrt(lax.optimization_barrier(jnp.mean(mixed * mixed, axis=-1, keepdims=True)) + EPSILON)
    first_read = (normed * norm_gain * jax.nn.silu(new_gate)).reshape(PROMPT_COUNT, HEADS * HEAD_DIM).astype(jnp.bfloat16)
    return (state_cache, first_read)
```

```python
import functools

import jax
import jax.numpy as jnp
from jax import lax
from jax.experimental import pallas as pl
from jax.experimental.pallas import tpu as pltpu
from jax.sharding import Mesh
from jax.sharding import PartitionSpec as P

HI, LO, Y, TP = "sp_hi", "sp_lo", "sp_y", "tp"
SP = (HI, LO, Y)
NEAR = (LO, Y)
EPSILON = 1e-06
F32, BF16 = jnp.float32, jnp.bfloat16


def in_three(x):
    high = x.astype(BF16)
    rest = x - high.astype(F32)
    middle = rest.astype(BF16)
    return high, middle, (rest - middle.astype(F32)).astype(BF16)


def state_kernel(
    prompt_ref, keep_ref, gap_ref, wf_ref, wv_ref, out_ref, x_buf, w_buf, p_sem, w_sem
):
    sequences, positions, width = prompt_ref.shape
    head = gap_ref.shape[1]
    peers = out_ref.shape[0]
    rows = head // peers
    pair = 2 * positions
    weights = [
        pltpu.make_async_copy(ref, w_buf.at[:, pl.ds(k * head, head)], w_sem.at[k])
        for k, ref in enumerate((wf_ref, wv_ref))
    ]
    chunks = [
        pltpu.make_async_copy(
            prompt_ref.at[pl.ds(2 * n, 2)], x_buf.at[pl.ds(2 * n, 2)], p_sem.at[n]
        )
        for n in range(sequences // 2)
    ]
    for copy in (*weights, *chunks):
        copy.start()
    keep = keep_ref[...]
    filler = jnp.ones((sequences, head - positions), F32)
    keep_columns = jnp.transpose(jnp.concatenate([keep, filler], axis=1))[:positions]
    log_columns = jnp.log(keep_columns)
    row = lax.broadcasted_iota(jnp.int32, (pair, pair), 0)
    column = lax.broadcasted_iota(jnp.int32, (pair, pair), 1)
    later_mask = (column > row) & (column // positions == row // positions)
    later_mask = later_mask.astype(F32).astype(BF16)
    gap = gap_ref[...]

    def spread(columns, n):
        return jnp.concatenate(
            [
                jnp.broadcast_to(columns[:, s : s + 1], (positions, head))
                for s in (2 * n, 2 * n + 1)
            ],
            axis=0,
        )

    for copy in weights:
        copy.wait()
    for n, copy in enumerate(chunks):
        copy.wait()
        x = x_buf[pl.ds(2 * n, 2)].reshape(pair, width)
        both = jnp.dot(x, w_buf[...], preferred_element_type=F32)
        values = both[:, head:].astype(BF16)
        loss = gap * jax.nn.sigmoid(-both[:, :head])
        keep_factor = spread(keep_columns, n)
        log_forget = spread(log_columns, n) + jnp.log1p(-loss)
        gate = (1.0 - keep_factor) + keep_factor * loss
        later = sum(
            jnp.dot(later_mask, part, preferred_element_type=F32)
            for part in in_three(log_forget)
        )
        gated = in_three(gate * jnp.exp(later))
        for k in range(2):
            s = 2 * n + k
            span = slice(k * positions, (k + 1) * positions)
            left = jnp.concatenate([part[span] for part in gated], axis=0)
            right = jnp.concatenate([values[span]] * 3, axis=0)
            state = lax.dot_general(
                left, right, (((0,), (0,)), ((), ())), preferred_element_type=F32
            )
            first = k * positions
            total = later[first : first + 1] + log_forget[first : first + 1]
            for j in range(peers):
                out_ref[j, s * rows : (s + 1) * rows, :] = state[j * rows : (j + 1) * rows]
                out_ref[j, head + s : head + s + 1, :] = total


def near_kernel(in_ref, out_ref, turned):
    blocks = in_ref.shape[0]
    sequences, _, head = out_ref.shape
    rows = head // blocks
    later = jnp.zeros((sequences, head), F32)
    factors = [None] * blocks
    for b in reversed(range(blocks)):
        factors[b] = jnp.exp(later)
        later = later + in_ref[b, head : head + sequences, :]
    rest = jnp.zeros((head - blocks * sequences, head), F32)
    turned[...] = jnp.transpose(jnp.concatenate([*factors, rest], axis=0))
    mine = turned[pl.ds(pl.multiple_of(lax.axis_index(NEAR) * rows, rows), rows), :]
    for s in range(sequences):
        total = jnp.zeros((rows, head), F32)
        for b in range(blocks):
            column = mine[:, b * sequences + s : b * sequences + s + 1]
            total = total + in_ref[b, s * rows : (s + 1) * rows, :] * column
        out_ref[s, :rows, :] = total
        out_ref[s, rows:, :] = later


def far_kernel(in_ref, weight_ref, state_ref, part_ref, turned):
    blocks = in_ref.shape[0]
    rows, head = state_ref.shape
    s = lax.axis_index(HI)
    later = jnp.zeros((1, head), F32)
    factors = [None] * blocks
    for b in reversed(range(blocks)):
        factors[b] = jnp.exp(later)
        later = later + in_ref[b, pl.ds(rows + s, 1), :]
    weight = weight_ref[pl.ds(s, 1), :]
    rest = jnp.zeros((head - blocks - 1, head), F32)
    turned[...] = jnp.transpose(jnp.concatenate([*factors, weight, rest], axis=0))
    mine = turned[pl.ds(pl.multiple_of(lax.axis_index(NEAR) * rows, rows), rows), :]
    total = jnp.zeros((rows, head), F32)
    for b in range(blocks):
        total = total + in_ref[b, :rows, :] * mine[:, b : b + 1]
    state_ref[...] = total.astype(state_ref.dtype)
    part = jnp.sum(total * mine[:, blocks : blocks + 1], axis=0, keepdims=True)
    part_ref[...] = jnp.broadcast_to(part, part_ref.shape)


def token_kernel(
    token_ref, wq_ref, wf_ref, wv_ref, wg_ref, gap_ref, gain_ref, weight_ref, own_ref, gate_ref
):
    token = jnp.concatenate([token_ref[k] for k in range(token_ref.shape[0])], axis=1)
    query, forget, value, gate = (
        jnp.dot(token, ref[...], preferred_element_type=F32)
        for ref in (wq_ref, wf_ref, wv_ref, wg_ref)
    )
    loss = gap_ref[...] * jax.nn.sigmoid(-forget)
    weight_ref[...] = query * (1.0 - loss)
    own = jnp.sum(query * loss, axis=1, keepdims=True)
    own_ref[...] = own * value.astype(BF16).astype(F32)
    gate_ref[...] = gain_ref[...] * (gate * jax.nn.sigmoid(gate))


def read_kernel(part_ref, own_ref, gate_ref, out_ref):
    sequences, head = own_ref.shape
    parts = part_ref[...].reshape(sequences, part_ref.shape[0] // sequences, head)
    mixed = jnp.sum(parts, axis=1) + own_ref[...]
    scale = lax.rsqrt(jnp.mean(mixed * mixed, axis=1, keepdims=True) + EPSILON)
    out_ref[...] = (mixed * scale * gate_ref[...]).astype(out_ref.dtype)


def cost(flops, bytes_accessed):
    return pl.CostEstimate(flops=flops, bytes_accessed=bytes_accessed, transcendentals=0)


ANY = pl.BlockSpec(memory_space=pl.ANY)
VMEM = pl.BlockSpec(memory_space=pltpu.VMEM)


def per_device(
    prompt, keep_scale, new_token, w_query, w_forget, w_value, w_outgate, floor_gap, norm_gain
):
    sequences, positions, width = prompt.shape
    head = norm_gain.shape[0]
    near = lax.axis_size(NEAR)
    far = lax.axis_size(HI)
    rows = head // near
    gap = floor_gap.reshape(1, head)
    gain = norm_gain.reshape(1, head)
    shaped = jax.ShapeDtypeStruct

    tp = lax.axis_size(TP)
    token = lax.all_to_all(
        jnp.broadcast_to(new_token[None], (tp, *new_token.shape)), TP, 0, 0, tiled=True
    )
    states = pl.pallas_call(
        state_kernel,
        out_shape=shaped((near, head + sequences, head), F32),
        in_specs=[ANY, VMEM, VMEM, ANY, ANY],
        out_specs=VMEM,
        scratch_shapes=[
            pltpu.VMEM(prompt.shape, BF16),
            pltpu.VMEM((width, 2 * head), BF16),
            pltpu.SemaphoreType.DMA((sequences // 2,)),
            pltpu.SemaphoreType.DMA((2,)),
        ],
        cost_estimate=cost(600_000_000, 4_000_000),
        name="block_states",
    )(prompt, keep_scale, gap, w_forget, w_value)
    states = lax.all_to_all(states, NEAR, 0, 0, tiled=True)
    states = pl.pallas_call(
        near_kernel,
        out_shape=shaped((far, rows + sequences, head), F32),
        in_specs=[VMEM],
        out_specs=VMEM,
        scratch_shapes=[pltpu.VMEM((head, head), F32)],
        cost_estimate=cost(1_000_000, 600_000),
        name="near_states",
    )(states)
    small = shaped((sequences, head), F32)
    weight, own, gate = pl.pallas_call(
        token_kernel,
        out_shape=(small, small, small),
        in_specs=[VMEM] * 7,
        out_specs=(VMEM,) * 3,
        cost_estimate=cost(20_000_000, 2_200_000),
        name="token",
    )(token, w_query, w_forget, w_value, w_outgate, gap, gain)
    states = lax.all_to_all(states, HI, 0, 0, tiled=True)
    final, part = pl.pallas_call(
        far_kernel,
        out_shape=(shaped((rows, head), BF16), shaped((near * far, head), F32)),
        in_specs=[VMEM] * 2,
        out_specs=(VMEM,) * 2,
        scratch_shapes=[pltpu.VMEM((head, head), F32)],
        cost_estimate=cost(1_000_000, 200_000),
        name="far_states",
    )(states, weight)
    part = lax.all_to_all(part[:, None, :], SP, 0, 0, tiled=True)[:, 0, :]
    first_read = pl.pallas_call(
        read_kernel,
        out_shape=shaped((sequences, head), BF16),
        in_specs=[VMEM] * 3,
        out_specs=VMEM,
        cost_estimate=cost(100_000, 40_000),
        name="read",
    )(part, own, gate)
    return final[None], first_read


def solution(mesh):
    finer = Mesh(mesh.devices.reshape(8, 2, 4, mesh.shape["tp"]), (HI, LO, Y, TP))
    placed = (
        P(None, SP, None),
        P(None, SP),
        P(None, TP),
        P(None, TP),
        P(None, TP),
        P(None, TP),
        P(None, TP),
        P(TP),
        P(),
    )
    return jax.shard_map(
        per_device,
        mesh=finer,
        in_specs=placed,
        out_specs=(P(TP, SP, None), P(None, TP)),
        check_vma=False,
    )
```

```python
import jax
import jax.numpy as jnp
from jax import lax
from jax.experimental import pallas as pl
from jax.experimental.pallas import tpu as pltpu
from jax.sharding import Mesh
from jax.sharding import PartitionSpec as P


HI, LO, Y, TP = "sp_hi", "sp_lo", "sp_y", "tp"
SP = (HI, LO, Y)
NEAR = (LO, Y)
EPSILON = 1e-06
F32, BF16 = jnp.float32, jnp.bfloat16


def in_three(x):
    high = x.astype(BF16)
    rest = x - high.astype(F32)
    middle = rest.astype(BF16)
    return high, middle, (rest - middle.astype(F32)).astype(BF16)


def state_kernel(
    prompt_ref, keep_ref, gap_ref, wf_ref, wv_ref, out_ref,
    x_buf, w_buf, keep_buf, gap_buf, both_buf, p_sem, w_sem, s_sem,
):
    sequences, positions, width = prompt_ref.shape
    head = gap_ref.shape[1]
    peers = out_ref.shape[0]
    rows = head // peers
    pair = 2 * positions
    weights = [
        pltpu.make_async_copy(ref, w_buf.at[:, pl.ds(k * head, head)], w_sem.at[k])
        for k, ref in enumerate((wf_ref, wv_ref))
    ]
    chunks = [
        pltpu.make_async_copy(
            prompt_ref.at[pl.ds(2 * n, 2)], x_buf.at[pl.ds(2 * n, 2)], p_sem.at[n]
        )
        for n in range(sequences // 2)
    ]
    smalls = [
        pltpu.make_async_copy(keep_ref, keep_buf, s_sem.at[0]),
        pltpu.make_async_copy(gap_ref, gap_buf, s_sem.at[1]),
    ]
    for copy in (*smalls, *weights, *chunks):
        copy.start()
    row = lax.broadcasted_iota(jnp.int32, (pair, pair), 0)
    column = lax.broadcasted_iota(jnp.int32, (pair, pair), 1)
    later_mask = (column > row) & (column // positions == row // positions)
    later_mask = later_mask.astype(F32).astype(BF16)
    for copy in smalls:
        copy.wait()
    keep = keep_buf[...]
    filler = jnp.ones((sequences, head - positions), F32)
    keep_columns = jnp.transpose(jnp.concatenate([keep, filler], axis=1))[:positions]
    log_columns = jnp.log(keep_columns)
    gap = gap_buf[...]

    def spread(columns, n):
        return jnp.concatenate(
            [
                jnp.broadcast_to(columns[:, s : s + 1], (positions, head))
                for s in (2 * n, 2 * n + 1)
            ],
            axis=0,
        )

    for copy in weights:
        copy.wait()
    for n, copy in enumerate(chunks):
        copy.wait()
        x = x_buf[pl.ds(2 * n, 2)].reshape(pair, width)
        both_buf[n] = jnp.dot(x, w_buf[...], preferred_element_type=F32)
    for n in range(sequences // 2):
        both = both_buf[n]
        values = both[:, head:].astype(BF16)
        loss = gap * jax.nn.sigmoid(-both[:, :head])
        keep_factor = spread(keep_columns, n)
        log_forget = spread(log_columns, n) + jnp.log1p(-loss)
        gate = (1.0 - keep_factor) + keep_factor * loss
        later = sum(
            jnp.dot(later_mask, part, preferred_element_type=F32)
            for part in in_three(log_forget)
        )
        gated = in_three(gate * jnp.exp(later))
        for k in range(2):
            s = 2 * n + k
            span = slice(k * positions, (k + 1) * positions)
            left = jnp.concatenate([part[span] for part in gated], axis=0)
            right = jnp.concatenate([values[span]] * 3, axis=0)
            state = lax.dot_general(
                left, right, (((0,), (0,)), ((), ())), preferred_element_type=F32
            )
            first = k * positions
            total = later[first : first + 1] + log_forget[first : first + 1]
            for j in range(peers):
                out_ref[j, s * rows : (s + 1) * rows, :] = state[j * rows : (j + 1) * rows]
                out_ref[j, head + s : head + s + 1, :] = total


def near_kernel(in_ref, out_ref, turned):
    blocks = in_ref.shape[0]
    sequences, _, head = out_ref.shape
    rows = head // blocks
    later = jnp.zeros((sequences, head), F32)
    factors = [None] * blocks
    for b in reversed(range(blocks)):
        factors[b] = jnp.exp(later)
        later = later + in_ref[b, head : head + sequences, :]
    rest = jnp.zeros((head - blocks * sequences, head), F32)
    turned[...] = jnp.transpose(jnp.concatenate([*factors, rest], axis=0))
    mine = turned[pl.ds(pl.multiple_of(lax.axis_index(NEAR) * rows, rows), rows), :]
    for s in range(sequences):
        total = jnp.zeros((rows, head), F32)
        for b in range(blocks):
            column = mine[:, b * sequences + s : b * sequences + s + 1]
            total = total + in_ref[b, s * rows : (s + 1) * rows, :] * column
        out_ref[s, :rows, :] = total
        out_ref[s, rows:, :] = later


def far_kernel(in_ref, weight_ref, state_ref, part_ref, turned):
    blocks = in_ref.shape[0]
    rows, head = state_ref.shape
    s = lax.axis_index(HI)
    later = jnp.zeros((1, head), F32)
    factors = [None] * blocks
    for b in reversed(range(blocks)):
        factors[b] = jnp.exp(later)
        later = later + in_ref[b, pl.ds(rows + s, 1), :]
    weight = weight_ref[pl.ds(s, 1), :]
    rest = jnp.zeros((head - blocks - 1, head), F32)
    turned[...] = jnp.transpose(jnp.concatenate([*factors, weight, rest], axis=0))
    mine = turned[pl.ds(pl.multiple_of(lax.axis_index(NEAR) * rows, rows), rows), :]
    total = jnp.zeros((rows, head), F32)
    for b in range(blocks):
        total = total + in_ref[b, :rows, :] * mine[:, b : b + 1]
    state_ref[...] = total.astype(state_ref.dtype)
    part = jnp.sum(total * mine[:, blocks : blocks + 1], axis=0, keepdims=True)
    part_ref[...] = jnp.broadcast_to(part, part_ref.shape)


def token_route(size, shift):
    if shift == 1:
        return [(i, i ^ 1) for i in range(size)]
    return [(i, (i + shift) % size) for i in range(size)]


def token_kernel(
    own_part, part_1, part_2, part_4, wq_ref, wf_ref, wv_ref, wg_ref, gap_ref, gain_ref,
    weight_ref, own_ref, gate_ref, token_buf,
):
    size = lax.axis_size(TP)
    me = lax.axis_index(TP)
    width = own_part.shape[1]
    parts = jnp.concatenate([own_part[...], part_1[...], part_2[...], part_4[...]], axis=1)
    parity = lax.rem(me, 2)
    for k in range(size):
        side = parity if k % 2 == 0 else 1 - parity
        owner = lax.rem((me - parity) + size - 2 * (k // 2), size) + side
        start = pl.multiple_of(owner * width, width)
        token_buf[:, pl.ds(start, width)] = parts[:, k * width : (k + 1) * width]
    token = token_buf[...]
    query, forget, value, gate = (
        jnp.dot(token, ref[...], preferred_element_type=F32)
        for ref in (wq_ref, wf_ref, wv_ref, wg_ref)
    )
    loss = gap_ref[...] * jax.nn.sigmoid(-forget)
    weight_ref[...] = query * (1.0 - loss)
    own = jnp.sum(query * loss, axis=1, keepdims=True)
    own_ref[...] = own * value.astype(BF16).astype(F32)
    gate_ref[...] = gain_ref[...] * (gate * jax.nn.sigmoid(gate))


def read_kernel(part_ref, own_ref, gate_ref, out_ref):
    sequences, head = own_ref.shape
    parts = part_ref[...].reshape(sequences, part_ref.shape[0] // sequences, head)
    mixed = jnp.sum(parts, axis=1) + own_ref[...]
    scale = lax.rsqrt(jnp.mean(mixed * mixed, axis=1, keepdims=True) + EPSILON)
    out_ref[...] = (mixed * scale * gate_ref[...]).astype(out_ref.dtype)


def cost(flops, bytes_accessed):
    return pl.CostEstimate(flops=flops, bytes_accessed=bytes_accessed, transcendentals=0)


def in_hbm(x):
    return pltpu.with_memory_space_constraint(x, pltpu.HBM)


HBM = pl.BlockSpec(memory_space=pltpu.HBM)
VMEM = pl.BlockSpec(memory_space=pltpu.VMEM)


def device_step(
    prompt, keep_scale, new_token, w_query, w_forget, w_value, w_outgate, floor_gap, norm_gain
):
    sequences, positions, width = prompt.shape
    head = norm_gain.shape[0]
    near = lax.axis_size(NEAR)
    far = lax.axis_size(HI)
    rows = head // near
    gap = floor_gap.reshape(1, head)
    gain = norm_gain.reshape(1, head)
    shaped = jax.ShapeDtypeStruct

    states = pl.pallas_call(
        state_kernel,
        out_shape=shaped((near, head + sequences, head), F32),
        in_specs=[HBM] * 5,
        out_specs=VMEM,
        scratch_shapes=[
            pltpu.VMEM(prompt.shape, BF16),
            pltpu.VMEM((width, 2 * head), BF16),
            pltpu.VMEM(keep_scale.shape, F32),
            pltpu.VMEM(gap.shape, F32),
            pltpu.VMEM((sequences // 2, 2 * positions, 2 * head), F32),
            pltpu.SemaphoreType.DMA((sequences // 2,)),
            pltpu.SemaphoreType.DMA((2,)),
            pltpu.SemaphoreType.DMA((2,)),
        ],
        cost_estimate=cost(600_000_000, 4_000_000),
        name="block_states",
        compiler_params=pltpu.CompilerParams(vmem_limit_bytes=8 << 20),
    )(*(in_hbm(x) for x in (prompt, keep_scale, gap, w_forget, w_value)))
    states = lax.all_to_all(states, NEAR, 0, 0, tiled=True)
    states = pl.pallas_call(
        near_kernel,
        out_shape=shaped((far, rows + sequences, head), F32),
        in_specs=[VMEM],
        out_specs=VMEM,
        scratch_shapes=[pltpu.VMEM((head, head), F32)],
        cost_estimate=cost(1_000_000, 600_000),
        name="near_states",
        compiler_params=pltpu.CompilerParams(vmem_limit_bytes=4 << 20),
    )(states)
    tp = lax.axis_size(TP)
    pieces = [new_token]
    for shift in (1, 2, 4):
        sent = pieces[0] if shift == 1 else jnp.concatenate(pieces, axis=1)
        pieces.append(lax.ppermute(sent, TP, token_route(tp, shift)))
    small = shaped((sequences, head), F32)
    weight, own, gate = pl.pallas_call(
        token_kernel,
        out_shape=(small, small, small),
        in_specs=[VMEM] * 10,
        out_specs=(VMEM,) * 3,
        scratch_shapes=[pltpu.VMEM((sequences, width), BF16)],
        cost_estimate=cost(20_000_000, 2_200_000),
        name="token",
        compiler_params=pltpu.CompilerParams(vmem_limit_bytes=6 << 20),
    )(*pieces, w_query, w_forget, w_value, w_outgate, gap, gain)
    states = lax.all_to_all(states, HI, 0, 0, tiled=True)
    final, part = pl.pallas_call(
        far_kernel,
        out_shape=(shaped((rows, head), BF16), shaped((near * far, head), F32)),
        in_specs=[VMEM] * 2,
        out_specs=(VMEM,) * 2,
        scratch_shapes=[pltpu.VMEM((head, head), F32)],
        cost_estimate=cost(1_000_000, 200_000),
        name="far_states",
        compiler_params=pltpu.CompilerParams(vmem_limit_bytes=2 << 20),
    )(states, weight)
    part = lax.all_to_all(part[:, None, :], SP, 0, 0, tiled=True)[:, 0, :]
    first_read = pl.pallas_call(
        read_kernel,
        out_shape=shaped((sequences, head), BF16),
        in_specs=[VMEM] * 3,
        out_specs=VMEM,
        cost_estimate=cost(100_000, 40_000),
        name="read",
        compiler_params=pltpu.CompilerParams(vmem_limit_bytes=1 << 20),
    )(part, own, gate)
    return final[None], first_read


def solution(mesh):
    finer = Mesh(mesh.devices.reshape(8, 2, 4, mesh.shape["tp"]), (HI, LO, Y, TP))
    placed = (
        P(None, SP, None),
        P(None, SP),
        P(None, TP),
        P(None, TP),
        P(None, TP),
        P(None, TP),
        P(None, TP),
        P(TP),
        P(),
    )
    return jax.shard_map(
        device_step,
        mesh=finer,
        in_specs=placed,
        out_specs=(P(TP, SP, None), P(None, TP)),
        check_vma=False,
    )
```

```python
import functools

import jax
import jax.numpy as jnp
from jax import lax
from jax.experimental import pallas as pl
from jax.experimental.pallas import tpu as pltpu
from jax.sharding import Mesh
from jax.sharding import PartitionSpec as P


HI, LO, Y, TP = "sp_hi", "sp_lo", "sp_y", "tp"
SP = (HI, LO, Y)
NEAR = (LO, Y)
EPSILON = 1e-06


def ring_from_middle(size):
    return [(size // 2 + k) % size for k in range(size)]


def near_order(low, y):
    return [l * y + m for l in range(low) for m in ring_from_middle(y)]


def read_order(far, near):
    return [h * len(near) + j for h in ring_from_middle(far) for j in near]


F32, BF16 = jnp.float32, jnp.bfloat16


def in_three(x):
    high = x.astype(BF16)
    rest = x - high.astype(F32)
    middle = rest.astype(BF16)
    return high, middle, (rest - middle.astype(F32)).astype(BF16)


def state_kernel(
    order, prompt_ref, keep_ref, gap_ref, wf_ref, wv_ref, out_ref,
    x_buf, w_buf, keep_buf, gap_buf, both_buf, p_sem, w_sem, s_sem,
):
    sequences, positions, width = prompt_ref.shape
    head = gap_ref.shape[1]
    peers = out_ref.shape[0]
    rows = head // peers
    pair = 2 * positions
    weights = [
        pltpu.make_async_copy(ref, w_buf.at[:, pl.ds(k * head, head)], w_sem.at[k])
        for k, ref in enumerate((wf_ref, wv_ref))
    ]
    chunks = [
        pltpu.make_async_copy(
            prompt_ref.at[pl.ds(2 * n, 2)], x_buf.at[pl.ds(2 * n, 2)], p_sem.at[n]
        )
        for n in range(sequences // 2)
    ]
    smalls = [
        pltpu.make_async_copy(keep_ref, keep_buf, s_sem.at[0]),
        pltpu.make_async_copy(gap_ref, gap_buf, s_sem.at[1]),
    ]
    for copy in (*smalls, *weights, *chunks):
        copy.start()
    row = lax.broadcasted_iota(jnp.int32, (pair, pair), 0)
    column = lax.broadcasted_iota(jnp.int32, (pair, pair), 1)
    later_mask = (column > row) & (column // positions == row // positions)
    later_mask = later_mask.astype(F32).astype(BF16)
    for copy in smalls:
        copy.wait()
    keep = keep_buf[...]
    filler = jnp.ones((sequences, head - positions), F32)
    keep_columns = jnp.transpose(jnp.concatenate([keep, filler], axis=1))[:positions]
    log_columns = jnp.log(keep_columns)
    gap = gap_buf[...]

    def spread(columns, n):
        return jnp.concatenate(
            [
                jnp.broadcast_to(columns[:, s : s + 1], (positions, head))
                for s in (2 * n, 2 * n + 1)
            ],
            axis=0,
        )

    for copy in weights:
        copy.wait()
    for n, copy in enumerate(chunks):
        copy.wait()
        x = x_buf[pl.ds(2 * n, 2)].reshape(pair, width)
        both_buf[n] = jnp.dot(x, w_buf[...], preferred_element_type=F32)
    for n in range(sequences // 2):
        both = both_buf[n]
        values = both[:, head:].astype(BF16)
        loss = gap * jax.nn.sigmoid(-both[:, :head])
        keep_factor = spread(keep_columns, n)
        log_forget = spread(log_columns, n) + jnp.log1p(-loss)
        gate = (1.0 - keep_factor) + keep_factor * loss
        later = sum(
            jnp.dot(later_mask, part, preferred_element_type=F32)
            for part in in_three(log_forget)
        )
        gated = in_three(gate * jnp.exp(later))
        for k in range(2):
            s = 2 * n + k
            span = slice(k * positions, (k + 1) * positions)
            left = jnp.concatenate([part[span] for part in gated], axis=0)
            right = jnp.concatenate([values[span]] * 3, axis=0)
            state = lax.dot_general(
                left, right, (((0,), (0,)), ((), ())), preferred_element_type=F32
            )
            first = k * positions
            total = later[first : first + 1] + log_forget[first : first + 1]
            for r, j in enumerate(order):
                out_ref[r, s * rows : (s + 1) * rows, :] = state[j * rows : (j + 1) * rows]
                out_ref[r, head + s : head + s + 1, :] = total


def near_kernel(order, far_ranks, in_ref, out_ref, turned):
    blocks = in_ref.shape[0]
    sequences, _, head = out_ref.shape
    rows = head // blocks
    later = jnp.zeros((sequences, head), F32)
    factors = [None] * blocks
    for b in reversed(range(blocks)):
        factors[b] = jnp.exp(later)
        later = later + in_ref[order.index(b), head : head + sequences, :]
    rest = jnp.zeros((head - blocks * sequences, head), F32)
    turned[...] = jnp.transpose(jnp.concatenate([*factors, rest], axis=0))
    mine = turned[pl.ds(pl.multiple_of(lax.axis_index(NEAR) * rows, rows), rows), :]
    for s in range(sequences):
        total = jnp.zeros((rows, head), F32)
        for b in range(blocks):
            column = mine[:, b * sequences + s : b * sequences + s + 1]
            total = total + in_ref[order.index(b), s * rows : (s + 1) * rows, :] * column
        out_ref[far_ranks.index(s), :rows, :] = total
        out_ref[far_ranks.index(s), rows:, :] = later


def far_kernel(order, in_ref, weight_ref, state_ref, part_ref, turned):
    blocks = in_ref.shape[0]
    rows, head = state_ref.shape
    s = lax.axis_index(HI)
    later = jnp.zeros((1, head), F32)
    factors = [None] * blocks
    for b in reversed(range(blocks)):
        factors[b] = jnp.exp(later)
        later = later + in_ref[order.index(b), pl.ds(rows + s, 1), :]
    weight = weight_ref[pl.ds(s, 1), :]
    rest = jnp.zeros((head - blocks - 1, head), F32)
    turned[...] = jnp.transpose(jnp.concatenate([*factors, weight, rest], axis=0))
    mine = turned[pl.ds(pl.multiple_of(lax.axis_index(NEAR) * rows, rows), rows), :]
    total = jnp.zeros((rows, head), F32)
    for b in range(blocks):
        total = total + in_ref[order.index(b), :rows, :] * mine[:, b : b + 1]
    state_ref[...] = total.astype(state_ref.dtype)
    part = jnp.sum(total * mine[:, blocks : blocks + 1], axis=0, keepdims=True)
    part_ref[...] = jnp.broadcast_to(part, part_ref.shape)


def token_route(size, shift):
    if shift == 1:
        return [(i, i ^ 1) for i in range(size)]
    return [(i, (i + shift) % size) for i in range(size)]


def token_kernel(
    same_ref, swapped_ref, wq_ref, wf_ref, wv_ref, wg_ref, gap_ref, gain_ref,
    weight_ref, own_ref, gate_ref, token_buf,
):
    size = lax.axis_size(TP)
    me = lax.axis_index(TP)
    width = token_buf.shape[1] // size
    for ref, core in ((same_ref, lax.rem(me, 2)), (swapped_ref, 1 - lax.rem(me, 2))):
        for k in range(size // 2):
            owner = lax.rem(me - lax.rem(me, 2) + size - 2 * k, size) + core
            start = pl.multiple_of(owner * width, width)
            token_buf[:, pl.ds(start, width)] = ref[:, k * width : (k + 1) * width]
    token = token_buf[...]
    query, forget, value, gate = (
        jnp.dot(token, ref[...], preferred_element_type=F32)
        for ref in (wq_ref, wf_ref, wv_ref, wg_ref)
    )
    loss = gap_ref[...] * jax.nn.sigmoid(-forget)
    weight_ref[...] = query * (1.0 - loss)
    own = jnp.sum(query * loss, axis=1, keepdims=True)
    own_ref[...] = own * value.astype(BF16).astype(F32)
    gate_ref[...] = gain_ref[...] * (gate * jax.nn.sigmoid(gate))


def read_kernel(part_ref, own_ref, gate_ref, out_ref):
    sequences, head = own_ref.shape
    parts = part_ref[...].reshape(sequences, part_ref.shape[0] // sequences, head)
    mixed = jnp.sum(parts, axis=1)
    half = sequences // 2
    mixed = jnp.concatenate([mixed[half:], mixed[:half]], axis=0) + own_ref[...]
    scale = lax.rsqrt(jnp.mean(mixed * mixed, axis=1, keepdims=True) + EPSILON)
    out_ref[...] = (mixed * scale * gate_ref[...]).astype(out_ref.dtype)


def cost(flops, bytes_accessed):
    return pl.CostEstimate(flops=flops, bytes_accessed=bytes_accessed, transcendentals=0)


def exchanged(x, axes, ranks):
    return lax.all_to_all(x, axes, 0, 0, tiled=True, axis_index_groups=[ranks])


def in_hbm(x):
    return pltpu.with_memory_space_constraint(x, pltpu.HBM)


HBM = pl.BlockSpec(memory_space=pltpu.HBM)
VMEM = pl.BlockSpec(memory_space=pltpu.VMEM)


def device_step(
    prompt, keep_scale, new_token, w_query, w_forget, w_value, w_outgate, floor_gap, norm_gain
):
    sequences, positions, width = prompt.shape
    head = norm_gain.shape[0]
    near = lax.axis_size(NEAR)
    far = lax.axis_size(HI)
    rows = head // near
    near_ranks = near_order(lax.axis_size(LO), lax.axis_size(Y))
    far_ranks = ring_from_middle(far)
    read_ranks = read_order(far, near_ranks)
    gap = floor_gap.reshape(1, head)
    gain = norm_gain.reshape(1, head)
    shaped = jax.ShapeDtypeStruct

    states = pl.pallas_call(
        functools.partial(state_kernel, near_ranks),
        out_shape=shaped((near, head + sequences, head), F32),
        in_specs=[HBM] * 5,
        out_specs=VMEM,
        scratch_shapes=[
            pltpu.VMEM(prompt.shape, BF16),
            pltpu.VMEM((width, 2 * head), BF16),
            pltpu.VMEM(keep_scale.shape, F32),
            pltpu.VMEM(gap.shape, F32),
            pltpu.VMEM((sequences // 2, 2 * positions, 2 * head), F32),
            pltpu.SemaphoreType.DMA((sequences // 2,)),
            pltpu.SemaphoreType.DMA((2,)),
            pltpu.SemaphoreType.DMA((2,)),
        ],
        cost_estimate=cost(600_000_000, 4_000_000),
        name="block_states",
        compiler_params=pltpu.CompilerParams(vmem_limit_bytes=8 << 20),
    )(*(in_hbm(x) for x in (prompt, keep_scale, gap, w_forget, w_value)))
    states = exchanged(states, NEAR, near_ranks)
    states = pl.pallas_call(
        functools.partial(near_kernel, near_ranks, far_ranks),
        out_shape=shaped((far, rows + sequences, head), F32),
        in_specs=[VMEM],
        out_specs=VMEM,
        scratch_shapes=[pltpu.VMEM((head, head), F32)],
        cost_estimate=cost(1_000_000, 600_000),
        name="near_states",
        compiler_params=pltpu.CompilerParams(vmem_limit_bytes=4 << 20),
    )(states)
    tp = lax.axis_size(TP)
    received = {}
    for shift in (2, 4, 6):
        received[shift] = lax.ppermute(new_token, TP, token_route(tp, shift))
    pieces = lax.optimization_barrier(jnp.concatenate([new_token, received[2]], axis=1))
    pieces = jnp.concatenate([pieces, received[4], received[6]], axis=1)
    swapped = lax.ppermute(pieces, TP, token_route(tp, 1))
    small = shaped((sequences, head), F32)
    weight, own, gate = pl.pallas_call(
        token_kernel,
        out_shape=(small, small, small),
        in_specs=[VMEM] * 8,
        out_specs=(VMEM,) * 3,
        scratch_shapes=[pltpu.VMEM((sequences, width), BF16)],
        cost_estimate=cost(20_000_000, 2_200_000),
        name="token",
        compiler_params=pltpu.CompilerParams(vmem_limit_bytes=6 << 20),
    )(pieces, swapped, w_query, w_forget, w_value, w_outgate, gap, gain)
    states = exchanged(states, HI, far_ranks)
    final, part = pl.pallas_call(
        functools.partial(far_kernel, far_ranks),
        out_shape=(shaped((rows, head), BF16), shaped((near * far, head), F32)),
        in_specs=[VMEM] * 2,
        out_specs=(VMEM,) * 2,
        scratch_shapes=[pltpu.VMEM((head, head), F32)],
        cost_estimate=cost(1_000_000, 200_000),
        name="far_states",
        compiler_params=pltpu.CompilerParams(vmem_limit_bytes=2 << 20),
    )(states, weight)
    part = exchanged(part[:, None, :], SP, read_ranks)[:, 0, :]
    first_read = pl.pallas_call(
        read_kernel,
        out_shape=shaped((sequences, head), BF16),
        in_specs=[VMEM] * 3,
        out_specs=VMEM,
        cost_estimate=cost(100_000, 40_000),
        name="read",
        compiler_params=pltpu.CompilerParams(vmem_limit_bytes=1 << 20),
    )(part, own, gate)
    return final[None], first_read


def solution(mesh):
    finer = Mesh(mesh.devices.reshape(8, 2, 4, mesh.shape["tp"]), (HI, LO, Y, TP))
    placed = (
        P(None, SP, None),
        P(None, SP),
        P(None, TP),
        P(None, TP),
        P(None, TP),
        P(None, TP),
        P(None, TP),
        P(TP),
        P(),
    )
    return jax.shard_map(
        device_step,
        mesh=finer,
        in_specs=placed,
        out_specs=(P(TP, SP, None), P(None, TP)),
        check_vma=False,
    )
```

```python
import functools

import jax
import jax.numpy as jnp
from jax import lax
from jax.experimental import pallas as pl
from jax.experimental.pallas import tpu as pltpu
from jax.sharding import Mesh
from jax.sharding import PartitionSpec as P

HI, LO, Y, TP = "sp_hi", "sp_lo", "sp_y", "tp"
SP = (HI, LO, Y)
NEAR = (LO, Y)
EPSILON = 1e-06


def ring_from_middle(size):
    return [(size // 2 + k) % size for k in range(size)]


def near_order(low, y):
    return [l * y + m for l in range(low) for m in ring_from_middle(y)]


def read_order(far, near):
    return [h * len(near) + j for h in ring_from_middle(far) for j in near]

F32, BF16 = jnp.float32, jnp.bfloat16


def in_two(x):
    high = x.astype(BF16)
    return high, (x - high.astype(F32)).astype(BF16)


def opening_kernel(out_ref):
    out_ref[...] = jnp.zeros_like(out_ref)


def state_kernel(
    order, opening_ref, prompt_ref, keep_ref, gap_ref, wf_ref, wv_ref, out_ref, total_ref, both_buf
):
    del opening_ref
    sequences, positions, width = prompt_ref.shape
    head = gap_ref.shape[1]
    peers = out_ref.shape[0]
    rows = head // peers
    pair = 2 * positions
    row = lax.broadcasted_iota(jnp.int32, (pair, pair), 0)
    column = lax.broadcasted_iota(jnp.int32, (pair, pair), 1)
    later_mask = (column > row) & (column // positions == row // positions)
    later_mask = later_mask.astype(F32).astype(BF16)
    filler = jnp.ones((sequences, head - positions), F32)
    keep_columns = jnp.transpose(jnp.concatenate([keep_ref[...], filler], axis=1))[:positions]
    log_columns = jnp.log(keep_columns)
    gap = gap_ref[...]

    def spread(columns, n):
        return jnp.concatenate(
            [
                jnp.broadcast_to(columns[:, s : s + 1], (positions, head))
                for s in (2 * n, 2 * n + 1)
            ],
            axis=0,
        )

    x = prompt_ref[...].reshape(sequences * positions, width)
    weights = jnp.concatenate([wf_ref[...], wv_ref[...]], axis=1)
    both_buf[...] = jnp.dot(x, weights, preferred_element_type=F32)
    for n in range(sequences // 2):
        both = both_buf[n * pair : (n + 1) * pair]
        values = both[:, head:].astype(BF16)
        loss = gap * jax.nn.sigmoid(-both[:, :head])
        keep_factor = spread(keep_columns, n)
        log_forget = spread(log_columns, n) + jnp.log1p(-loss)
        gate = (1.0 - keep_factor) + keep_factor * loss
        later = sum(
            jnp.dot(later_mask, part, preferred_element_type=F32)
            for part in in_two(log_forget)
        )
        gated = in_two(gate * jnp.exp(later))
        for k in range(2):
            s = 2 * n + k
            span = slice(k * positions, (k + 1) * positions)
            left = jnp.concatenate([part[span] for part in gated], axis=0)
            right = jnp.concatenate([values[span]] * 2, axis=0)
            state = lax.dot_general(
                left, right, (((0,), (0,)), ((), ())), preferred_element_type=F32
            )
            first = k * positions
            total_ref[s : s + 1, :] = later[first : first + 1] + log_forget[first : first + 1]
            for r, j in enumerate(order):
                out_ref[r, s * rows : (s + 1) * rows, :] = state[j * rows : (j + 1) * rows]


def token_route(near, tp):
    return [
        (j * tp + (i + j) % tp, j * tp + i) for j in range(near) for i in range(tp)
    ]


def chunk_of_lane(shape, rows):
    return lax.broadcasted_iota(jnp.int32, shape, len(shape) - 1) // rows


def token_kernel(
    order, token_ref, totals_ref, wq_ref, wf_ref, wv_ref, wg_ref, states_ref, out_ref,
    tile_buf, sem,
):
    del states_ref
    size = lax.axis_size(TP)
    width = token_ref.shape[1]
    peers, tile_rows, head = tile_buf.shape
    rows = head // peers
    block = lax.rem(lax.axis_index(TP) + lax.axis_index(NEAR), size)
    span = pl.ds(pl.multiple_of(block * width, width), width)
    token = token_ref[...]
    picked = lax.broadcasted_iota(jnp.int32, (token.shape[0], 1), 0) == lax.axis_index(HI)
    tile = []
    for ref in (wq_ref, wf_ref, wv_ref, wg_ref):
        part = jnp.dot(token, ref[span, :], preferred_element_type=F32)
        part = jnp.sum(jnp.where(picked, part, 0.0), axis=0, keepdims=True)
        tile += [part, pltpu.roll(part, rows, 1)]
    tile = jnp.concatenate(tile, axis=0)
    totals = totals_ref[...]
    chunk = chunk_of_lane(tile.shape, rows)
    for r, j in enumerate(order):
        tile_buf[r] = jnp.where(chunk == j, totals, tile)
    last = pl.ds(out_ref.shape[1] - tile_rows, tile_rows)
    copy = pltpu.make_async_copy(tile_buf, out_ref.at[:, last], sem)
    copy.start()
    copy.wait()


def near_kernel(order, far_ranks, in_ref, gap_ref, gain_ref, out_ref, token_ref, turned):
    blocks = in_ref.shape[0]
    sequences, _, head = out_ref.shape
    rows = head // blocks
    later = jnp.zeros((sequences, head), F32)
    factors = [None] * blocks
    for b in reversed(range(blocks)):
        factors[b] = jnp.exp(later)
        later = later + in_ref[order.index(b), head : head + sequences, :]
    rest = jnp.zeros((head - blocks * sequences, head), F32)
    turned[...] = jnp.transpose(jnp.concatenate([*factors, rest], axis=0))
    mine = turned[pl.ds(pl.multiple_of(lax.axis_index(NEAR) * rows, rows), rows), :]
    for s in range(sequences):
        total = jnp.zeros((rows, head), F32)
        for b in range(blocks):
            column = mine[:, b * sequences + s : b * sequences + s + 1]
            total = total + in_ref[order.index(b), s * rows : (s + 1) * rows, :] * column
        out_ref[far_ranks.index(s), :rows, :] = total
        out_ref[far_ranks.index(s), rows : rows + 1, :] = later[s : s + 1]
    tiles = sum(in_ref[b, head:, :] for b in range(blocks))
    own_chunk = chunk_of_lane((1, head), rows) == lax.axis_index(NEAR)
    query, forget, value, gate = (
        jnp.where(
            own_chunk,
            pltpu.roll(tiles[2 * k + 1 : 2 * k + 2], head - rows, 1),
            tiles[2 * k : 2 * k + 1],
        )
        for k in range(4)
    )
    loss = gap_ref[...] * jax.nn.sigmoid(-forget)
    own = jnp.sum(query * loss, axis=1, keepdims=True) * value.astype(BF16).astype(F32)
    own = jnp.where(lax.axis_index(NEAR) == 0, own, 0.0)
    token_ref[...] = jnp.concatenate(
        [query * (1.0 - loss), own, jnp.zeros((sequences - 2, head), F32)], axis=0
    )
    gate = gain_ref[...] * (gate * jax.nn.sigmoid(gate))
    spare = jnp.zeros((sequences - 2, head), F32)
    for r in range(sequences):
        out_ref[r, rows + 1 :, :] = jnp.concatenate([gate, spare], axis=0)


def far_kernel(order, in_ref, token_ref, state_ref, part_ref, gate_ref, turned):
    blocks = in_ref.shape[0]
    rows, head = state_ref.shape
    later = jnp.zeros((1, head), F32)
    factors = [None] * blocks
    for b in reversed(range(blocks)):
        factors[b] = jnp.exp(later)
        later = later + in_ref[order.index(b), rows : rows + 1, :]
        gate_ref[b : b + 1, :] = in_ref[order.index(b), rows + 1 : rows + 2, :]
    weight, own = (token_ref[k : k + 1, :] for k in range(2))
    rest = jnp.zeros((head - blocks - 1, head), F32)
    turned[...] = jnp.transpose(jnp.concatenate([*factors, weight, rest], axis=0))
    mine = turned[pl.ds(pl.multiple_of(lax.axis_index(NEAR) * rows, rows), rows), :]
    total = jnp.zeros((rows, head), F32)
    for b in range(blocks):
        total = total + in_ref[order.index(b), :rows, :] * mine[:, b : b + 1]
    state_ref[...] = total.astype(state_ref.dtype)
    part = jnp.sum(total * mine[:, blocks : blocks + 1], axis=0, keepdims=True) + own
    part_ref[...] = jnp.broadcast_to(part, part_ref.shape)


def read_kernel(part_ref, gate_ref, out_ref):
    sequences, head = out_ref.shape
    parts = part_ref[...].reshape(sequences, part_ref.shape[0] // sequences, head)
    mixed = jnp.sum(parts, axis=1)
    half = sequences // 2
    mixed = jnp.concatenate([mixed[half:], mixed[:half]], axis=0)
    scale = lax.rsqrt(jnp.mean(mixed * mixed, axis=1, keepdims=True) + EPSILON)
    out_ref[...] = (mixed * scale * gate_ref[...]).astype(out_ref.dtype)


def cost(flops, bytes_accessed):
    return pl.CostEstimate(flops=flops, bytes_accessed=bytes_accessed, transcendentals=0)


def exchanged(x, axes, ranks):
    return lax.all_to_all(x, axes, 0, 0, tiled=True, axis_index_groups=[ranks])


ANY = pl.BlockSpec(memory_space=pl.ANY)
VMEM = pl.BlockSpec(memory_space=pltpu.VMEM)


def per_device(
    prompt, keep_scale, new_token, w_query, w_forget, w_value, w_outgate, floor_gap, norm_gain
):
    sequences, positions, width = prompt.shape
    head = norm_gain.shape[0]
    near = lax.axis_size(NEAR)
    far = lax.axis_size(HI)
    rows = head // near
    near_ranks = near_order(lax.axis_size(LO), lax.axis_size(Y))
    far_ranks = ring_from_middle(far)
    read_ranks = read_order(far, near_ranks)
    gap = floor_gap.reshape(1, head)
    gain = norm_gain.reshape(1, head)
    shaped = jax.ShapeDtypeStruct

    head_start = pl.pallas_call(
        opening_kernel,
        out_shape=shaped((8, head), F32),
        out_specs=VMEM,
        cost_estimate=cost(20_000_000_000, 40_000_000),
        name="opening",
        compiler_params=pltpu.CompilerParams(vmem_limit_bytes=1 << 20),
    )()
    new_token, head_start = lax.optimization_barrier((new_token, head_start))
    token = lax.ppermute(new_token, (*NEAR, TP), token_route(near, lax.axis_size(TP)))
    states, totals = pl.pallas_call(
        functools.partial(state_kernel, near_ranks),
        out_shape=(
            shaped((near, head + sequences, head), F32),
            shaped((sequences, head), F32),
        ),
        in_specs=[VMEM] * 6,
        out_specs=(VMEM,) * 2,
        scratch_shapes=[pltpu.VMEM((sequences * positions, 2 * head), F32)],
        cost_estimate=cost(600_000_000, 4_000_000),
        name="block_states",
        compiler_params=pltpu.CompilerParams(vmem_limit_bytes=8 << 20),
    )(head_start, prompt, keep_scale, gap, w_forget, w_value)
    states = pl.pallas_call(
        functools.partial(token_kernel, near_ranks),
        out_shape=shaped(states.shape, F32),
        in_specs=[VMEM] * 6 + [ANY],
        out_specs=ANY,
        scratch_shapes=[pltpu.VMEM((near, sequences, head), F32), pltpu.SemaphoreType.DMA],
        input_output_aliases={6: 0},
        cost_estimate=cost(2_000_000, 300_000),
        name="token",
        compiler_params=pltpu.CompilerParams(vmem_limit_bytes=6 << 20),
    )(token, totals, w_query, w_forget, w_value, w_outgate, states)
    states = exchanged(states, NEAR, near_ranks)
    states, token_rows = pl.pallas_call(
        functools.partial(near_kernel, near_ranks, far_ranks),
        out_shape=(
            shaped((far, rows + sequences, head), F32),
            shaped((sequences, head), F32),
        ),
        in_specs=[VMEM] * 3,
        out_specs=(VMEM,) * 2,
        scratch_shapes=[pltpu.VMEM((head, head), F32)],
        cost_estimate=cost(1_000_000, 600_000),
        name="near_states",
        compiler_params=pltpu.CompilerParams(vmem_limit_bytes=4 << 20),
    )(states, gap, gain)
    states = exchanged(states, HI, far_ranks)
    final, part, gate = pl.pallas_call(
        functools.partial(far_kernel, far_ranks),
        out_shape=(
            shaped((rows, head), BF16),
            shaped((near * far, head), F32),
            shaped((sequences, head), F32),
        ),
        in_specs=[VMEM] * 2,
        out_specs=(VMEM,) * 3,
        scratch_shapes=[pltpu.VMEM((head, head), F32)],
        cost_estimate=cost(1_000_000, 200_000),
        name="far_states",
        compiler_params=pltpu.CompilerParams(vmem_limit_bytes=2 << 20),
    )(states, token_rows)
    part = exchanged(part[:, None, :], SP, read_ranks)[:, 0, :]
    first_read = pl.pallas_call(
        read_kernel,
        out_shape=shaped((sequences, head), BF16),
        in_specs=[VMEM] * 2,
        out_specs=VMEM,
        cost_estimate=cost(100_000, 40_000),
        name="read",
        compiler_params=pltpu.CompilerParams(vmem_limit_bytes=1 << 20),
    )(part, gate)
    return final[None], first_read


def solution(mesh):
    finer = Mesh(mesh.devices.reshape(8, 2, 4, mesh.shape["tp"]), (HI, LO, Y, TP))
    placed = (
        P(None, SP, None),
        P(None, SP),
        P(None, TP),
        P(None, TP),
        P(None, TP),
        P(None, TP),
        P(None, TP),
        P(TP),
        P(),
    )
    return jax.shard_map(
        per_device,
        mesh=finer,
        in_specs=placed,
        out_specs=(P(TP, SP, None), P(None, TP)),
        check_vma=False,
    )
```

```python
import functools

import jax
import jax.numpy as jnp
from jax import lax
from jax.experimental import pallas as pl
from jax.experimental.pallas import tpu as pltpu
from jax.sharding import Mesh
from jax.sharding import PartitionSpec as P

HI, LO, Y, TP = "sp_hi", "sp_lo", "sp_y", "tp"
SP = (HI, LO, Y)
NEAR = (LO, Y)
EPSILON = 1e-06


FAR_ORDER, READ_ORDER, Y_ORDER = (4, 0, 7, 1, 6, 2, 5, 3), (4, 0, 7, 1, 6, 2, 5, 3), (2, 3, 0, 1)


F32, BF16 = jnp.float32, jnp.bfloat16


def near_order(low):
    return [l * len(Y_ORDER) + m for l in range(low) for m in Y_ORDER]


def read_order(near):
    return [h * len(near) + j for h in READ_ORDER for j in near]


def in_two(x):
    high = x.astype(BF16)
    return high, (x - high.astype(F32)).astype(BF16)


def opening_kernel(out_ref):
    out_ref[...] = jnp.zeros_like(out_ref)


def state_kernel(
    order, opening_ref, prompt_ref, keep_ref, gap_ref, wf_ref, wv_ref, out_ref, both_buf
):
    del opening_ref
    sequences, positions, width = prompt_ref.shape
    head = gap_ref.shape[1]
    peers = out_ref.shape[0]
    rows = head // peers
    pair = 2 * positions
    row = lax.broadcasted_iota(jnp.int32, (pair, pair), 0)
    column = lax.broadcasted_iota(jnp.int32, (pair, pair), 1)
    later_mask = (column > row) & (column // positions == row // positions)
    later_mask = later_mask.astype(F32).astype(BF16)
    filler = jnp.ones((sequences, head - positions), F32)
    keep_columns = jnp.transpose(jnp.concatenate([keep_ref[...], filler], axis=1))[:positions]
    log_columns = jnp.log(keep_columns)
    gap = gap_ref[...]

    def spread(columns, n):
        return jnp.concatenate(
            [
                jnp.broadcast_to(columns[:, s : s + 1], (positions, head))
                for s in (2 * n, 2 * n + 1)
            ],
            axis=0,
        )

    x = prompt_ref[...].reshape(sequences * positions, width)
    weights = jnp.concatenate([wf_ref[...], wv_ref[...]], axis=1)
    both_buf[...] = jnp.dot(x, weights, preferred_element_type=F32)
    for n in range(sequences // 2):
        both = both_buf[n * pair : (n + 1) * pair]
        values = both[:, head:].astype(BF16)
        loss = gap * jax.nn.sigmoid(-both[:, :head])
        keep_factor = spread(keep_columns, n)
        log_forget = spread(log_columns, n) + jnp.log1p(-loss)
        gate = (1.0 - keep_factor) + keep_factor * loss
        later = sum(
            jnp.dot(later_mask, part, preferred_element_type=F32)
            for part in in_two(log_forget)
        )
        gated = in_two(gate * jnp.exp(later))
        for k in range(2):
            s = 2 * n + k
            span = slice(k * positions, (k + 1) * positions)
            left = jnp.concatenate([part[span] for part in gated], axis=0)
            right = jnp.concatenate([values[span]] * 2, axis=0)
            state = lax.dot_general(
                left, right, (((0,), (0,)), ((), ())), preferred_element_type=F32
            )
            first = k * positions
            total = later[first : first + 1] + log_forget[first : first + 1]
            for r, j in enumerate(order):
                out_ref[r, s * rows : (s + 1) * rows, :] = state[j * rows : (j + 1) * rows]
                out_ref[r, head + s : head + s + 1, :] = total


def token_route(far, tp):
    return [(h * tp + (i + h) % tp, h * tp + i) for h in range(far) for i in range(tp)]


def near_kernel(
    order, far_ranks, in_ref, token_ref, wq_ref, wf_ref, wv_ref, wg_ref, out_ref, turned
):
    blocks = in_ref.shape[0]
    sequences, _, head = out_ref.shape
    rows = head // blocks
    width = token_ref.shape[1]
    block = lax.rem(lax.axis_index(TP) + lax.axis_index(HI), lax.axis_size(TP))
    span = pl.ds(pl.multiple_of(block * width, width), width)
    token = token_ref[...]
    parts = [
        jnp.dot(token, ref[span, :], preferred_element_type=F32)
        for ref in (wq_ref, wf_ref, wv_ref, wg_ref)
    ]
    later = jnp.zeros((sequences, head), F32)
    factors = [None] * blocks
    for b in reversed(range(blocks)):
        factors[b] = jnp.exp(later)
        later = later + in_ref[order.index(b), head : head + sequences, :]
    rest = jnp.zeros((head - blocks * sequences, head), F32)
    turned[...] = jnp.transpose(jnp.concatenate([*factors, rest], axis=0))
    mine = turned[pl.ds(pl.multiple_of(lax.axis_index(NEAR) * rows, rows), rows), :]
    spare = jnp.zeros((sequences - 1 - len(parts), head), F32)
    for s in range(sequences):
        total = jnp.zeros((rows, head), F32)
        for b in range(blocks):
            column = mine[:, b * sequences + s : b * sequences + s + 1]
            total = total + in_ref[order.index(b), s * rows : (s + 1) * rows, :] * column
        out_ref[far_ranks.index(s), :rows, :] = total
        out_ref[far_ranks.index(s), rows:, :] = jnp.concatenate(
            [later[s : s + 1], *(part[s : s + 1] for part in parts), spare], axis=0
        )


def far_kernel(order, in_ref, gap_ref, gain_ref, state_ref, part_ref, turned):
    blocks = in_ref.shape[0]
    rows, head = state_ref.shape
    later = jnp.zeros((1, head), F32)
    factors = [None] * blocks
    for b in reversed(range(blocks)):
        factors[b] = jnp.exp(later)
        later = later + in_ref[order.index(b), rows : rows + 1, :]
    tile = sum(in_ref[b, rows:, :] for b in range(blocks))
    query, forget, value, gate = (tile[k : k + 1] for k in range(1, 5))
    loss = gap_ref[...] * jax.nn.sigmoid(-forget)
    own = jnp.sum(query * loss, axis=1, keepdims=True) * value.astype(BF16).astype(F32)
    gate = gain_ref[...] * (gate * jax.nn.sigmoid(gate))
    weight = query * (1.0 - loss)
    rest = jnp.zeros((head - blocks - 1, head), F32)
    turned[...] = jnp.transpose(jnp.concatenate([*factors, weight, rest], axis=0))
    mine = turned[pl.ds(pl.multiple_of(lax.axis_index(NEAR) * rows, rows), rows), :]
    total = jnp.zeros((rows, head), F32)
    for b in range(blocks):
        total = total + in_ref[order.index(b), :rows, :] * mine[:, b : b + 1]
    state_ref[...] = total.astype(state_ref.dtype)
    part = jnp.sum(total * mine[:, blocks : blocks + 1], axis=0, keepdims=True)
    part = part + jnp.where(lax.axis_index(NEAR) == 0, own, 0.0)
    row = lax.broadcasted_iota(jnp.int32, part_ref.shape, 0)
    part_ref[...] = jnp.where(lax.rem(row, 2) == 0, part, gate)


def read_kernel(part_ref, state_ref, out_ref, cache_ref):
    cache_ref[...] = state_ref[...]
    sequences, head = out_ref.shape
    parts = part_ref[...].reshape(sequences, part_ref.shape[0] // sequences, head)
    row = lax.broadcasted_iota(jnp.int32, parts.shape, 1)
    mixed = jnp.sum(jnp.where(lax.rem(row, 2) == 0, parts, 0.0), axis=1)
    scale = lax.rsqrt(jnp.mean(mixed * mixed, axis=1, keepdims=True) + EPSILON)
    read = mixed * scale * parts[:, 1, :]
    places = [READ_ORDER.index(s) for s in range(sequences)]
    read = jnp.concatenate([read[a : a + 1] for a in places], axis=0)
    out_ref[...] = read.astype(out_ref.dtype)


def cost(flops, bytes_accessed):
    return pl.CostEstimate(flops=flops, bytes_accessed=bytes_accessed, transcendentals=0)


def exchanged(x, axes, ranks):
    return lax.all_to_all(x, axes, 0, 0, tiled=True, axis_index_groups=[ranks])


VMEM = pl.BlockSpec(memory_space=pltpu.VMEM)


def per_device(
    prompt, keep_scale, new_token, w_query, w_forget, w_value, w_outgate, floor_gap, norm_gain
):
    sequences, positions, width = prompt.shape
    head = norm_gain.shape[0]
    near = lax.axis_size(NEAR)
    far = lax.axis_size(HI)
    rows = head // near
    near_ranks = near_order(lax.axis_size(LO))
    far_ranks = list(FAR_ORDER)
    read_ranks = read_order(near_ranks)
    gap = floor_gap.reshape(1, head)
    gain = norm_gain.reshape(1, head)
    shaped = jax.ShapeDtypeStruct

    head_start = pl.pallas_call(
        opening_kernel,
        out_shape=shaped((8, head), F32),
        out_specs=VMEM,
        cost_estimate=cost(20_000_000_000, 40_000_000),
        name="opening",
        compiler_params=pltpu.CompilerParams(vmem_limit_bytes=1 << 20),
    )()
    token = lax.ppermute(new_token, (HI, TP), token_route(far, lax.axis_size(TP)))
    states = pl.pallas_call(
        functools.partial(state_kernel, near_ranks),
        out_shape=shaped((near, head + sequences, head), F32),
        in_specs=[VMEM] * 6,
        out_specs=VMEM,
        scratch_shapes=[pltpu.VMEM((sequences * positions, 2 * head), F32)],
        cost_estimate=cost(600_000_000, 4_000_000),
        name="block_states",
        compiler_params=pltpu.CompilerParams(vmem_limit_bytes=8 << 20),
    )(head_start, prompt, keep_scale, gap, w_forget, w_value)
    states = exchanged(states, NEAR, near_ranks)
    states = pl.pallas_call(
        functools.partial(near_kernel, near_ranks, far_ranks),
        out_shape=shaped((far, rows + sequences, head), F32),
        in_specs=[VMEM] * 6,
        out_specs=VMEM,
        scratch_shapes=[pltpu.VMEM((head, head), F32)],
        cost_estimate=cost(20_000_000, 2_600_000),
        name="near_states",
        compiler_params=pltpu.CompilerParams(vmem_limit_bytes=6 << 20),
    )(states, token, w_query, w_forget, w_value, w_outgate)
    states = exchanged(states, HI, far_ranks)
    final, part = pl.pallas_call(
        functools.partial(far_kernel, far_ranks),
        out_shape=(shaped((rows, head), BF16), shaped((2 * near * far, head), F32)),
        in_specs=[VMEM] * 3,
        out_specs=(VMEM,) * 2,
        scratch_shapes=[pltpu.VMEM((head, head), F32)],
        cost_estimate=cost(1_000_000, 200_000),
        name="far_states",
        compiler_params=pltpu.CompilerParams(vmem_limit_bytes=2 << 20),
    )(states, gap, gain)
    part = exchanged(part.reshape(near * far, 2, head), SP, read_ranks).reshape(part.shape)
    first_read, cache = pl.pallas_call(
        read_kernel,
        out_shape=(shaped((sequences, head), BF16), shaped((rows, head), BF16)),
        in_specs=[VMEM] * 2,
        out_specs=(VMEM,) * 2,
        cost_estimate=cost(100_000, 40_000),
        name="read",
        compiler_params=pltpu.CompilerParams(vmem_limit_bytes=1 << 20),
    )(part, final)
    return cache[None], first_read


def solution(mesh):
    finer = Mesh(mesh.devices.reshape(8, 2, 4, mesh.shape["tp"]), (HI, LO, Y, TP))
    placed = (
        P(None, SP, None),
        P(None, SP),
        P(None, TP),
        P(None, TP),
        P(None, TP),
        P(None, TP),
        P(None, TP),
        P(TP),
        P(),
    )
    return jax.shard_map(
        per_device,
        mesh=finer,
        in_specs=placed,
        out_specs=(P(TP, SP, None), P(None, TP)),
        check_vma=False,
    )
```

```python
import functools

import jax
import jax.numpy as jnp
from jax import lax
from jax.experimental import pallas as pl
from jax.experimental.pallas import tpu as pltpu
from jax.sharding import Mesh
from jax.sharding import PartitionSpec as P

HI, LO, Y, TP = "sp_hi", "sp_lo", "sp_y", "tp"
SP = (HI, LO, Y)
NEAR = (LO, Y)
EPSILON = 1e-06
F32, BF16 = jnp.float32, jnp.bfloat16
FAR_ORDER = READ_ORDER = (4, 0, 7, 1, 6, 2, 5, 3)
NEAR_ORDER = (2, 0, 3, 1, 6, 4, 7, 5)


def read_order(near):
    return [h * len(near) + j for h in READ_ORDER for j in near]


def in_two(x):
    high = x.astype(BF16)
    return high, (x - high.astype(F32)).astype(BF16)


def opening_kernel(out_ref):
    out_ref[...] = jnp.zeros_like(out_ref)


def state_kernel(
    order, opening_ref, prompt_ref, keep_ref, gap_ref, wf_ref, wv_ref, out_ref, both_buf
):
    del opening_ref
    sequences, positions, width = prompt_ref.shape
    head = gap_ref.shape[1]
    peers = out_ref.shape[0]
    rows = head // peers
    pair = 2 * positions
    row = lax.broadcasted_iota(jnp.int32, (pair, pair), 0)
    column = lax.broadcasted_iota(jnp.int32, (pair, pair), 1)
    later_mask = (column > row) & (column // positions == row // positions)
    later_mask = later_mask.astype(F32).astype(BF16)
    filler = jnp.ones((sequences, head - positions), F32)
    keep_columns = jnp.transpose(jnp.concatenate([keep_ref[...], filler], axis=1))[:positions]
    log_columns = jnp.log(keep_columns)
    gap = gap_ref[...]

    def spread(columns, n):
        return jnp.concatenate(
            [
                jnp.broadcast_to(columns[:, s : s + 1], (positions, head))
                for s in (2 * n, 2 * n + 1)
            ],
            axis=0,
        )

    x = prompt_ref[...].reshape(sequences * positions, width)
    weights = jnp.concatenate([wf_ref[...], wv_ref[...]], axis=1)
    both_buf[...] = jnp.dot(x, weights, preferred_element_type=F32)
    for n in range(sequences // 2):
        both = both_buf[n * pair : (n + 1) * pair]
        values = both[:, head:].astype(BF16)
        loss = gap * jax.nn.sigmoid(-both[:, :head])
        keep_factor = spread(keep_columns, n)
        log_forget = spread(log_columns, n) + jnp.log1p(-loss)
        gate = (1.0 - keep_factor) + keep_factor * loss
        later = sum(
            jnp.dot(later_mask, part, preferred_element_type=F32)
            for part in in_two(log_forget)
        )
        gated = in_two(gate * jnp.exp(later))
        for k in range(2):
            s = 2 * n + k
            span = slice(k * positions, (k + 1) * positions)
            left = jnp.concatenate([part[span] for part in gated], axis=0)
            right = jnp.concatenate([values[span]] * 2, axis=0)
            state = lax.dot_general(
                left, right, (((0,), (0,)), ((), ())), preferred_element_type=F32
            )
            first = k * positions
            total = later[first : first + 1] + log_forget[first : first + 1]
            for r, j in enumerate(order):
                out_ref[r, s * rows : (s + 1) * rows, :] = state[j * rows : (j + 1) * rows]
                out_ref[r, head + s : head + s + 1, :] = total


def token_route(far, tp):
    return [(h * tp + (i + h) % tp, h * tp + i) for h in range(far) for i in range(tp)]


def near_kernel(
    order, far_ranks, in_ref, token_ref, wq_ref, wf_ref, wv_ref, wg_ref, out_ref, turned
):
    blocks = in_ref.shape[0]
    sequences, _, head = out_ref.shape
    rows = head // blocks
    width = token_ref.shape[1]
    block = lax.rem(lax.axis_index(TP) + lax.axis_index(HI), lax.axis_size(TP))
    span = pl.ds(pl.multiple_of(block * width, width), width)
    token = token_ref[...]
    parts = [
        jnp.dot(token, ref[span, :], preferred_element_type=F32)
        for ref in (wq_ref, wf_ref, wv_ref, wg_ref)
    ]
    later = jnp.zeros((sequences, head), F32)
    factors = [None] * blocks
    for b in reversed(range(blocks)):
        factors[b] = jnp.exp(later)
        later = later + in_ref[order.index(b), head : head + sequences, :]
    rest = jnp.zeros((head - blocks * sequences, head), F32)
    turned[...] = jnp.transpose(jnp.concatenate([*factors, rest], axis=0))
    mine = turned[pl.ds(pl.multiple_of(lax.axis_index(NEAR) * rows, rows), rows), :]
    spare = jnp.zeros((sequences - 1 - len(parts), head), F32)
    for s in range(sequences):
        total = jnp.zeros((rows, head), F32)
        for b in range(blocks):
            column = mine[:, b * sequences + s : b * sequences + s + 1]
            total = total + in_ref[order.index(b), s * rows : (s + 1) * rows, :] * column
        out_ref[far_ranks.index(s), :rows, :] = total
        out_ref[far_ranks.index(s), rows:, :] = jnp.concatenate(
            [later[s : s + 1], *(part[s : s + 1] for part in parts), spare], axis=0
        )


def far_kernel(order, in_ref, gap_ref, gain_ref, state_ref, part_ref, turned):
    blocks = in_ref.shape[0]
    rows, head = state_ref.shape
    later = jnp.zeros((1, head), F32)
    factors = [None] * blocks
    for b in reversed(range(blocks)):
        factors[b] = jnp.exp(later)
        later = later + in_ref[order.index(b), rows : rows + 1, :]
    tile = sum(in_ref[b, rows:, :] for b in range(blocks))
    query, forget, value, gate = (tile[k : k + 1] for k in range(1, 5))
    loss = gap_ref[...] * jax.nn.sigmoid(-forget)
    own = jnp.sum(query * loss, axis=1, keepdims=True) * value.astype(BF16).astype(F32)
    gate = gain_ref[...] * (gate * jax.nn.sigmoid(gate))
    weight = query * (1.0 - loss)
    rest = jnp.zeros((head - blocks - 1, head), F32)
    turned[...] = jnp.transpose(jnp.concatenate([*factors, weight, rest], axis=0))
    mine = turned[pl.ds(pl.multiple_of(lax.axis_index(NEAR) * rows, rows), rows), :]
    total = jnp.zeros((rows, head), F32)
    for b in range(blocks):
        total = total + in_ref[order.index(b), :rows, :] * mine[:, b : b + 1]
    state_ref[...] = total.astype(state_ref.dtype)
    part = jnp.sum(total * mine[:, blocks : blocks + 1], axis=0, keepdims=True)
    part = part + jnp.where(lax.axis_index(NEAR) == 0, own, 0.0)
    row = lax.broadcasted_iota(jnp.int32, part_ref.shape, 0)
    part_ref[...] = jnp.where(lax.rem(row, 2) == 0, part, gate)


def read_kernel(part_ref, state_ref, out_ref, cache_ref):
    cache_ref[...] = state_ref[...]
    sequences, head = out_ref.shape
    parts = part_ref[...].reshape(sequences, part_ref.shape[0] // sequences, head)
    row = lax.broadcasted_iota(jnp.int32, parts.shape, 1)
    mixed = jnp.sum(jnp.where(lax.rem(row, 2) == 0, parts, 0.0), axis=1)
    scale = lax.rsqrt(jnp.mean(mixed * mixed, axis=1, keepdims=True) + EPSILON)
    read = mixed * scale * parts[:, 1, :]
    places = [READ_ORDER.index(s) for s in range(sequences)]
    read = jnp.concatenate([read[a : a + 1] for a in places], axis=0)
    out_ref[...] = read.astype(out_ref.dtype)


def cost(flops, bytes_accessed):
    return pl.CostEstimate(flops=flops, bytes_accessed=bytes_accessed, transcendentals=0)


def exchanged(x, axes, ranks):
    return lax.all_to_all(x, axes, 0, 0, tiled=True, axis_index_groups=[ranks])


VMEM = pl.BlockSpec(memory_space=pltpu.VMEM)


def per_device(
    prompt, keep_scale, new_token, w_query, w_forget, w_value, w_outgate, floor_gap, norm_gain
):
    sequences, positions, width = prompt.shape
    head = norm_gain.shape[0]
    near = lax.axis_size(NEAR)
    far = lax.axis_size(HI)
    rows = head // near
    near_ranks = list(NEAR_ORDER)
    far_ranks = list(FAR_ORDER)
    read_ranks = read_order(near_ranks)
    gap = floor_gap.reshape(1, head)
    gain = norm_gain.reshape(1, head)
    shaped = jax.ShapeDtypeStruct

    head_start = pl.pallas_call(
        opening_kernel,
        out_shape=shaped((8, head), F32),
        out_specs=VMEM,
        cost_estimate=cost(20_000_000_000, 40_000_000),
        name="opening",
        compiler_params=pltpu.CompilerParams(vmem_limit_bytes=1 << 20),
    )()
    token = lax.ppermute(new_token, (HI, TP), token_route(far, lax.axis_size(TP)))
    states = pl.pallas_call(
        functools.partial(state_kernel, near_ranks),
        out_shape=shaped((near, head + sequences, head), F32),
        in_specs=[VMEM] * 6,
        out_specs=VMEM,
        scratch_shapes=[pltpu.VMEM((sequences * positions, 2 * head), F32)],
        cost_estimate=cost(600_000_000, 4_000_000),
        name="block_states",
        compiler_params=pltpu.CompilerParams(vmem_limit_bytes=8 << 20),
    )(head_start, prompt, keep_scale, gap, w_forget, w_value)
    states = exchanged(states, NEAR, near_ranks)
    states = pl.pallas_call(
        functools.partial(near_kernel, near_ranks, far_ranks),
        out_shape=shaped((far, rows + sequences, head), F32),
        in_specs=[VMEM] * 6,
        out_specs=VMEM,
        scratch_shapes=[pltpu.VMEM((head, head), F32)],
        cost_estimate=cost(20_000_000, 2_600_000),
        name="near_states",
        compiler_params=pltpu.CompilerParams(vmem_limit_bytes=6 << 20),
    )(states, token, w_query, w_forget, w_value, w_outgate)
    states = exchanged(states, HI, far_ranks)
    final, part = pl.pallas_call(
        functools.partial(far_kernel, far_ranks),
        out_shape=(shaped((rows, head), BF16), shaped((2 * near * far, head), F32)),
        in_specs=[VMEM] * 3,
        out_specs=(VMEM,) * 2,
        scratch_shapes=[pltpu.VMEM((head, head), F32)],
        cost_estimate=cost(1_000_000, 200_000),
        name="far_states",
        compiler_params=pltpu.CompilerParams(vmem_limit_bytes=2 << 20),
    )(states, gap, gain)
    part = exchanged(part.reshape(near * far, 1, 2 * head), SP, read_ranks).reshape(part.shape)
    first_read, cache = pl.pallas_call(
        read_kernel,
        out_shape=(shaped((sequences, head), BF16), shaped((rows, head), BF16)),
        in_specs=[VMEM] * 2,
        out_specs=(VMEM,) * 2,
        cost_estimate=cost(100_000, 40_000),
        name="read",
        compiler_params=pltpu.CompilerParams(vmem_limit_bytes=1 << 20),
    )(part, final)
    return cache[None], first_read


def solution(mesh):
    finer = Mesh(mesh.devices.reshape(8, 2, 4, mesh.shape["tp"]), (HI, LO, Y, TP))
    placed = (
        P(None, SP, None),
        P(None, SP),
        P(None, TP),
        P(None, TP),
        P(None, TP),
        P(None, TP),
        P(None, TP),
        P(TP),
        P(),
    )
    return jax.shard_map(
        per_device,
        mesh=finer,
        in_specs=placed,
        out_specs=(P(TP, SP, None), P(None, TP)),
        check_vma=False,
    )
```

```python
import functools

import jax
import jax.numpy as jnp
from jax import lax
from jax.experimental import pallas as pl
from jax.experimental.pallas import tpu as pltpu
from jax.sharding import Mesh
from jax.sharding import PartitionSpec as P


HI, LO, Y, TP = "sp_hi", "sp_lo", "sp_y", "tp"
SP = (HI, LO, Y)
NEAR = (LO, Y)
EPSILON = 1e-06
F32, BF16 = jnp.float32, jnp.bfloat16
FAR_ORDER = READ_ORDER = (4, 0, 7, 1, 6, 2, 5, 3)
NEAR_ORDER = (2, 0, 3, 1, 6, 4, 7, 5)


def read_order(near):
    return [h * len(near) + j for h in READ_ORDER for j in near]


def in_two(x):
    high = x.astype(BF16)
    return high, (x - high.astype(F32)).astype(BF16)


def opening_kernel(out_ref):
    out_ref[...] = jnp.zeros_like(out_ref)


def state_kernel(
    order, opening_ref, prompt_ref, keep_ref, gap_ref, wf_ref, wv_ref, out_ref, both_buf
):
    del opening_ref
    sequences, positions, width = prompt_ref.shape
    head = gap_ref.shape[1]
    peers = out_ref.shape[0]
    rows = head // peers
    pair = 2 * positions
    row = lax.broadcasted_iota(jnp.int32, (pair, pair), 0)
    column = lax.broadcasted_iota(jnp.int32, (pair, pair), 1)
    later_mask = (column > row) & (column // positions == row // positions)
    later_mask = later_mask.astype(F32).astype(BF16)
    filler = jnp.ones((sequences, head - positions), F32)
    keep_columns = jnp.transpose(jnp.concatenate([keep_ref[...], filler], axis=1))[:positions]
    log_columns = jnp.log(keep_columns)
    gap = gap_ref[...]

    def spread(columns, n):
        return jnp.concatenate(
            [
                jnp.broadcast_to(columns[:, s : s + 1], (positions, head))
                for s in (2 * n, 2 * n + 1)
            ],
            axis=0,
        )

    x = prompt_ref[...].reshape(sequences * positions, width)
    weights = jnp.concatenate([wf_ref[...], wv_ref[...]], axis=1)
    both_buf[...] = jnp.dot(x, weights, preferred_element_type=F32)
    for n in range(sequences // 2):
        both = both_buf[n * pair : (n + 1) * pair]
        values = both[:, head:].astype(BF16)
        loss = gap * jax.nn.sigmoid(-both[:, :head])
        keep_factor = spread(keep_columns, n)
        log_forget = spread(log_columns, n) + jnp.log1p(-loss)
        gate = (1.0 - keep_factor) + keep_factor * loss
        later = sum(
            jnp.dot(later_mask, part, preferred_element_type=F32)
            for part in in_two(log_forget)
        )
        gated = in_two(gate * jnp.exp(later))
        for k in range(2):
            s = 2 * n + k
            span = slice(k * positions, (k + 1) * positions)
            left = jnp.concatenate([part[span] for part in gated], axis=0)
            right = jnp.concatenate([values[span]] * 2, axis=0)
            state = lax.dot_general(
                left, right, (((0,), (0,)), ((), ())), preferred_element_type=F32
            )
            first = k * positions
            total = later[first : first + 1] + log_forget[first : first + 1]
            for r, j in enumerate(order):
                out_ref[r, s * rows : (s + 1) * rows, :] = state[j * rows : (j + 1) * rows]
                out_ref[r, head + s : head + s + 1, :] = total


def token_route(far, tp):
    return [(h * tp + (i ^ h ^ (tp - 1)), h * tp + i) for h in range(far) for i in range(tp)]


def near_kernel(order, far_ranks, in_ref, out_ref, later_ref, turned):
    blocks = in_ref.shape[0]
    sequences, _, head = out_ref.shape
    rows = head // blocks
    later = jnp.zeros((sequences, head), F32)
    factors = [None] * blocks
    for b in reversed(range(blocks)):
        factors[b] = jnp.exp(later)
        later = later + in_ref[order.index(b), head : head + sequences, :]
    rest = jnp.zeros((head - blocks * sequences, head), F32)
    turned[...] = jnp.transpose(jnp.concatenate([*factors, rest], axis=0))
    mine = turned[pl.ds(pl.multiple_of(lax.axis_index(NEAR) * rows, rows), rows), :]
    later_ref[...] = later
    for s in range(sequences):
        total = jnp.zeros((rows, head), F32)
        for b in range(blocks):
            column = mine[:, b * sequences + s : b * sequences + s + 1]
            total = total + in_ref[order.index(b), s * rows : (s + 1) * rows, :] * column
        out_ref[far_ranks.index(s), :rows, :] = total


def token_kernel(
    far_ranks, token_ref, later_ref, wq_ref, wf_ref, wv_ref, wg_ref, states_ref, out_ref,
    tile_buf, sem,
):
    del states_ref
    width = token_ref.shape[1]
    block = lax.axis_index(TP) ^ lax.axis_index(HI) ^ (lax.axis_size(TP) - 1)
    span = pl.ds(pl.multiple_of(block * width, width), width)
    token = token_ref[...]
    parts = [later_ref[...]] + [
        jnp.dot(token, ref[span, :], preferred_element_type=F32)
        for ref in (wq_ref, wf_ref, wv_ref, wg_ref)
    ]
    targets, tile_rows, head = tile_buf.shape
    spare = jnp.zeros((tile_rows - len(parts), head), F32)
    for s in range(targets):
        tile_buf[far_ranks.index(s)] = jnp.concatenate(
            [*(part[s : s + 1] for part in parts), spare], axis=0
        )
    last = pl.ds(out_ref.shape[1] - tile_rows, tile_rows)
    copy = pltpu.make_async_copy(tile_buf, out_ref.at[:, last], sem)
    copy.start()
    copy.wait()


def far_kernel(order, in_ref, gap_ref, gain_ref, state_ref, part_ref, turned):
    blocks = in_ref.shape[0]
    rows, head = state_ref.shape
    later = jnp.zeros((1, head), F32)
    factors = [None] * blocks
    for b in reversed(range(blocks)):
        factors[b] = jnp.exp(later)
        later = later + in_ref[order.index(b), rows : rows + 1, :]
    tile = sum(in_ref[b, rows:, :] for b in range(blocks))
    query, forget, value, gate = (tile[k : k + 1] for k in range(1, 5))
    loss = gap_ref[...] * jax.nn.sigmoid(-forget)
    own = jnp.sum(query * loss, axis=1, keepdims=True) * value.astype(BF16).astype(F32)
    gate = gain_ref[...] * (gate * jax.nn.sigmoid(gate))
    weight = query * (1.0 - loss)
    rest = jnp.zeros((head - blocks - 1, head), F32)
    turned[...] = jnp.transpose(jnp.concatenate([*factors, weight, rest], axis=0))
    mine = turned[pl.ds(pl.multiple_of(lax.axis_index(NEAR) * rows, rows), rows), :]
    total = jnp.zeros((rows, head), F32)
    for b in range(blocks):
        total = total + in_ref[order.index(b), :rows, :] * mine[:, b : b + 1]
    state_ref[...] = total.astype(state_ref.dtype)
    part = jnp.sum(total * mine[:, blocks : blocks + 1], axis=0, keepdims=True)
    part = part + jnp.where(lax.axis_index(NEAR) == 0, own, 0.0)
    row = lax.broadcasted_iota(jnp.int32, part_ref.shape, 0)
    part_ref[...] = jnp.where(lax.rem(row, 2) == 0, part, gate)


def read_kernel(part_ref, state_ref, out_ref, cache_ref):
    cache_ref[...] = state_ref[...]
    sequences, head = out_ref.shape
    parts = part_ref[...].reshape(sequences, part_ref.shape[0] // sequences, head)
    row = lax.broadcasted_iota(jnp.int32, parts.shape, 1)
    mixed = jnp.sum(jnp.where(lax.rem(row, 2) == 0, parts, 0.0), axis=1)
    scale = lax.rsqrt(jnp.mean(mixed * mixed, axis=1, keepdims=True) + EPSILON)
    read = mixed * scale * parts[:, 1, :]
    places = [READ_ORDER.index(s) for s in range(sequences)]
    read = jnp.concatenate([read[a : a + 1] for a in places], axis=0)
    out_ref[...] = read.astype(out_ref.dtype)


def cost(flops, bytes_accessed):
    return pl.CostEstimate(flops=flops, bytes_accessed=bytes_accessed, transcendentals=0)


def exchanged(x, axes, ranks):
    return lax.all_to_all(x, axes, 0, 0, tiled=True, axis_index_groups=[ranks])


ANY = pl.BlockSpec(memory_space=pl.ANY)
VMEM = pl.BlockSpec(memory_space=pltpu.VMEM)


def device_step(
    prompt, keep_scale, new_token, w_query, w_forget, w_value, w_outgate, floor_gap, norm_gain
):
    sequences, positions, _ = prompt.shape
    head = norm_gain.shape[0]
    near = lax.axis_size(NEAR)
    far = lax.axis_size(HI)
    rows = head // near
    near_ranks = list(NEAR_ORDER)
    far_ranks = list(FAR_ORDER)
    read_ranks = read_order(near_ranks)
    gap = floor_gap.reshape(1, head)
    gain = norm_gain.reshape(1, head)
    shaped = jax.ShapeDtypeStruct

    head_start = pl.pallas_call(
        opening_kernel,
        out_shape=shaped((8, head), F32),
        out_specs=VMEM,
        cost_estimate=cost(20_000_000_000, 40_000_000),
        name="opening",
        compiler_params=pltpu.CompilerParams(vmem_limit_bytes=1 << 20),
    )()
    token = lax.ppermute(new_token, (HI, TP), token_route(far, lax.axis_size(TP)))
    states = pl.pallas_call(
        functools.partial(state_kernel, near_ranks),
        out_shape=shaped((near, head + sequences, head), F32),
        in_specs=[VMEM] * 6,
        out_specs=VMEM,
        scratch_shapes=[pltpu.VMEM((sequences * positions, 2 * head), F32)],
        cost_estimate=cost(600_000_000, 4_000_000),
        name="block_states",
        compiler_params=pltpu.CompilerParams(vmem_limit_bytes=8 << 20),
    )(head_start, prompt, keep_scale, gap, w_forget, w_value)
    states = exchanged(states, NEAR, near_ranks)
    states, later = pl.pallas_call(
        functools.partial(near_kernel, near_ranks, far_ranks),
        out_shape=(
            shaped((far, rows + sequences, head), F32),
            shaped((sequences, head), F32),
        ),
        in_specs=[VMEM],
        out_specs=(VMEM,) * 2,
        scratch_shapes=[pltpu.VMEM((head, head), F32)],
        cost_estimate=cost(1_000_000, 600_000),
        name="near_states",
        compiler_params=pltpu.CompilerParams(vmem_limit_bytes=2 << 20),
    )(states)
    states = pl.pallas_call(
        functools.partial(token_kernel, far_ranks),
        out_shape=shaped(states.shape, F32),
        in_specs=[VMEM] * 6 + [ANY],
        out_specs=ANY,
        scratch_shapes=[pltpu.VMEM((far, sequences, head), F32), pltpu.SemaphoreType.DMA],
        input_output_aliases={6: 0},
        cost_estimate=cost(20_000_000, 2_200_000),
        name="token",
        compiler_params=pltpu.CompilerParams(vmem_limit_bytes=6 << 20),
    )(token, later, w_query, w_forget, w_value, w_outgate, states)
    states = exchanged(states, HI, far_ranks)
    final, part = pl.pallas_call(
        functools.partial(far_kernel, far_ranks),
        out_shape=(shaped((rows, head), BF16), shaped((2 * near * far, head), F32)),
        in_specs=[VMEM] * 3,
        out_specs=(VMEM,) * 2,
        scratch_shapes=[pltpu.VMEM((head, head), F32)],
        cost_estimate=cost(1_000_000, 200_000),
        name="far_states",
        compiler_params=pltpu.CompilerParams(vmem_limit_bytes=2 << 20),
    )(states, gap, gain)
    part = exchanged(part.reshape(near * far, 1, 2 * head), SP, read_ranks).reshape(part.shape)
    first_read, cache = pl.pallas_call(
        read_kernel,
        out_shape=(shaped((sequences, head), BF16), shaped((rows, head), BF16)),
        in_specs=[VMEM] * 2,
        out_specs=(VMEM,) * 2,
        cost_estimate=cost(100_000, 40_000),
        name="read",
        compiler_params=pltpu.CompilerParams(vmem_limit_bytes=1 << 20),
    )(part, final)
    return cache[None], first_read


def solution(mesh):
    finer = Mesh(mesh.devices.reshape(8, 2, 4, mesh.shape["tp"]), (HI, LO, Y, TP))
    placed = (
        P(None, SP, None),
        P(None, SP),
        P(None, TP),
        P(None, TP),
        P(None, TP),
        P(None, TP),
        P(None, TP),
        P(TP),
        P(),
    )
    return jax.shard_map(
        device_step,
        mesh=finer,
        in_specs=placed,
        out_specs=(P(TP, SP, None), P(None, TP)),
        check_vma=False,
    )
```

```python
import functools

import jax
import jax.numpy as jnp
from jax import lax
from jax.experimental import pallas as pl
from jax.experimental.pallas import tpu as pltpu
from jax.sharding import Mesh
from jax.sharding import PartitionSpec as P


HI, LO, Y, TP = "sp_hi", "sp_lo", "sp_y", "tp"
SP = (HI, LO, Y)
NEAR = (LO, Y)
EPSILON = 1e-06
F32, BF16 = jnp.float32, jnp.bfloat16
FAR_ORDER = READ_ORDER = (4, 0, 7, 1, 6, 2, 5, 3)
NEAR_ORDER = (2, 0, 3, 1, 6, 4, 7, 5)


def read_order(near):
    return [h * len(near) + j for h in READ_ORDER for j in near]


def in_two(x):
    high = x.astype(BF16)
    return high, (x - high.astype(F32)).astype(BF16)


def opening_kernel(out_ref):
    out_ref[...] = jnp.zeros_like(out_ref)


def state_kernel(
    order, opening_ref, prompt_ref, keep_ref, gap_ref, wf_ref, wv_ref, out_ref, both_buf
):
    del opening_ref
    sequences, positions, width = prompt_ref.shape
    head = gap_ref.shape[1]
    peers = out_ref.shape[0]
    rows = head // peers
    pair = 2 * positions
    row = lax.broadcasted_iota(jnp.int32, (pair, pair), 0)
    column = lax.broadcasted_iota(jnp.int32, (pair, pair), 1)
    later_mask = (column > row) & (column // positions == row // positions)
    later_mask = later_mask.astype(F32).astype(BF16)
    filler = jnp.ones((sequences, head - positions), F32)
    keep_columns = jnp.transpose(jnp.concatenate([keep_ref[...], filler], axis=1))[:positions]
    log_columns = jnp.log(keep_columns)
    gap = gap_ref[...]

    def spread(columns, n):
        return jnp.concatenate(
            [
                jnp.broadcast_to(columns[:, s : s + 1], (positions, head))
                for s in (2 * n, 2 * n + 1)
            ],
            axis=0,
        )

    x = prompt_ref[...].reshape(sequences * positions, width)
    weights = jnp.concatenate([wf_ref[...], wv_ref[...]], axis=1)
    both_buf[...] = jnp.dot(x, weights, preferred_element_type=F32)
    for n in range(sequences // 2):
        both = both_buf[n * pair : (n + 1) * pair]
        values = both[:, head:].astype(BF16)
        loss = gap * jax.nn.sigmoid(-both[:, :head])
        keep_factor = spread(keep_columns, n)
        log_forget = spread(log_columns, n) + jnp.log1p(-loss)
        gate = (1.0 - keep_factor) + keep_factor * loss
        later = sum(
            jnp.dot(later_mask, part, preferred_element_type=F32)
            for part in in_two(log_forget)
        )
        gated = in_two(gate * jnp.exp(later))
        for k in range(2):
            s = 2 * n + k
            span = slice(k * positions, (k + 1) * positions)
            left = jnp.concatenate([part[span] for part in gated], axis=0)
            right = jnp.concatenate([values[span]] * 2, axis=0)
            state = lax.dot_general(
                left, right, (((0,), (0,)), ((), ())), preferred_element_type=F32
            )
            first = k * positions
            total = later[first : first + 1] + log_forget[first : first + 1]
            for r, j in enumerate(order):
                out_ref[r, s * rows : (s + 1) * rows, :] = state[j * rows : (j + 1) * rows]
                out_ref[r, head + s : head + s + 1, :] = total


def route_mask(h, far):
    return h ^ (far - 1) ^ (2 * (h < far // 2))


def token_route(far, tp):
    return [(h * tp + (i ^ route_mask(h, far)), h * tp + i) for h in range(far) for i in range(tp)]


def near_kernel(order, far_ranks, in_ref, out_ref, later_ref, turned):
    blocks = in_ref.shape[0]
    sequences, _, head = out_ref.shape
    rows = head // blocks
    later = jnp.zeros((sequences, head), F32)
    factors = [None] * blocks
    for b in reversed(range(blocks)):
        factors[b] = jnp.exp(later)
        later = later + in_ref[order.index(b), head : head + sequences, :]
    rest = jnp.zeros((head - blocks * sequences, head), F32)
    turned[...] = jnp.transpose(jnp.concatenate([*factors, rest], axis=0))
    mine = turned[pl.ds(pl.multiple_of(lax.axis_index(NEAR) * rows, rows), rows), :]
    later_ref[...] = later
    for s in range(sequences):
        total = jnp.zeros((rows, head), F32)
        for b in range(blocks):
            column = mine[:, b * sequences + s : b * sequences + s + 1]
            total = total + in_ref[order.index(b), s * rows : (s + 1) * rows, :] * column
        out_ref[far_ranks.index(s), :rows, :] = total


def token_kernel(
    far_ranks, token_ref, later_ref, wq_ref, wf_ref, wv_ref, wg_ref, states_ref, out_ref,
    tile_buf, sem,
):
    del states_ref
    width = token_ref.shape[1]
    block = lax.axis_index(TP) ^ route_mask(lax.axis_index(HI), lax.axis_size(HI))
    span = pl.ds(pl.multiple_of(block * width, width), width)
    token = token_ref[...]
    parts = [later_ref[...]] + [
        jnp.dot(token, ref[span, :], preferred_element_type=F32)
        for ref in (wq_ref, wf_ref, wv_ref, wg_ref)
    ]
    targets, tile_rows, head = tile_buf.shape
    spare = jnp.zeros((tile_rows - len(parts), head), F32)
    for s in range(targets):
        tile_buf[far_ranks.index(s)] = jnp.concatenate(
            [*(part[s : s + 1] for part in parts), spare], axis=0
        )
    last = pl.ds(out_ref.shape[1] - tile_rows, tile_rows)
    copy = pltpu.make_async_copy(tile_buf, out_ref.at[:, last], sem)
    copy.start()
    copy.wait()


def far_kernel(order, in_ref, gap_ref, gain_ref, state_ref, part_ref, turned):
    blocks = in_ref.shape[0]
    rows, head = state_ref.shape
    later = jnp.zeros((1, head), F32)
    factors = [None] * blocks
    for b in reversed(range(blocks)):
        factors[b] = jnp.exp(later)
        later = later + in_ref[order.index(b), rows : rows + 1, :]
    tile = sum(in_ref[b, rows:, :] for b in range(blocks))
    query, forget, value, gate = (tile[k : k + 1] for k in range(1, 5))
    loss = gap_ref[...] * jax.nn.sigmoid(-forget)
    own = jnp.sum(query * loss, axis=1, keepdims=True) * value.astype(BF16).astype(F32)
    gate = gain_ref[...] * (gate * jax.nn.sigmoid(gate))
    weight = query * (1.0 - loss)
    rest = jnp.zeros((head - blocks - 1, head), F32)
    turned[...] = jnp.transpose(jnp.concatenate([*factors, weight, rest], axis=0))
    mine = turned[pl.ds(pl.multiple_of(lax.axis_index(NEAR) * rows, rows), rows), :]
    total = jnp.zeros((rows, head), F32)
    for b in range(blocks):
        total = total + in_ref[order.index(b), :rows, :] * mine[:, b : b + 1]
    state_ref[...] = total.astype(state_ref.dtype)
    part = jnp.sum(total * mine[:, blocks : blocks + 1], axis=0, keepdims=True)
    part = part + jnp.where(lax.axis_index(NEAR) == 0, own, 0.0)
    row = lax.broadcasted_iota(jnp.int32, part_ref.shape, 0)
    part_ref[...] = jnp.where(lax.rem(row, 2) == 0, part, gate)


def read_kernel(part_ref, state_ref, out_ref, cache_ref):
    cache_ref[...] = state_ref[...]
    sequences, head = out_ref.shape
    parts = part_ref[...].reshape(sequences, part_ref.shape[0] // sequences, head)
    row = lax.broadcasted_iota(jnp.int32, parts.shape, 1)
    mixed = jnp.sum(jnp.where(lax.rem(row, 2) == 0, parts, 0.0), axis=1)
    scale = lax.rsqrt(jnp.mean(mixed * mixed, axis=1, keepdims=True) + EPSILON)
    read = mixed * scale * parts[:, 1, :]
    places = [READ_ORDER.index(s) for s in range(sequences)]
    read = jnp.concatenate([read[a : a + 1] for a in places], axis=0)
    out_ref[...] = read.astype(out_ref.dtype)


def cost(flops, bytes_accessed):
    return pl.CostEstimate(flops=flops, bytes_accessed=bytes_accessed, transcendentals=0)


def exchanged(x, axes, ranks):
    return lax.all_to_all(x, axes, 0, 0, tiled=True, axis_index_groups=[ranks])


ANY = pl.BlockSpec(memory_space=pl.ANY)
VMEM = pl.BlockSpec(memory_space=pltpu.VMEM)


def device_step(
    prompt, keep_scale, new_token, w_query, w_forget, w_value, w_outgate, floor_gap, norm_gain
):
    sequences, positions, _ = prompt.shape
    head = norm_gain.shape[0]
    near = lax.axis_size(NEAR)
    far = lax.axis_size(HI)
    rows = head // near
    near_ranks = list(NEAR_ORDER)
    far_ranks = list(FAR_ORDER)
    read_ranks = read_order(near_ranks)
    gap = floor_gap.reshape(1, head)
    gain = norm_gain.reshape(1, head)
    shaped = jax.ShapeDtypeStruct

    head_start = pl.pallas_call(
        opening_kernel,
        out_shape=shaped((8, head), F32),
        out_specs=VMEM,
        cost_estimate=cost(20_000_000_000, 40_000_000),
        name="opening",
        compiler_params=pltpu.CompilerParams(vmem_limit_bytes=1 << 20),
    )()
    token = lax.ppermute(new_token, (HI, TP), token_route(far, lax.axis_size(TP)))
    states = pl.pallas_call(
        functools.partial(state_kernel, near_ranks),
        out_shape=shaped((near, head + sequences, head), F32),
        in_specs=[VMEM] * 6,
        out_specs=VMEM,
        scratch_shapes=[pltpu.VMEM((sequences * positions, 2 * head), F32)],
        cost_estimate=cost(600_000_000, 4_000_000),
        name="block_states",
        compiler_params=pltpu.CompilerParams(vmem_limit_bytes=8 << 20),
    )(head_start, prompt, keep_scale, gap, w_forget, w_value)
    states = exchanged(states, NEAR, near_ranks)
    states, later = pl.pallas_call(
        functools.partial(near_kernel, near_ranks, far_ranks),
        out_shape=(
            shaped((far, rows + sequences, head), F32),
            shaped((sequences, head), F32),
        ),
        in_specs=[VMEM],
        out_specs=(VMEM,) * 2,
        scratch_shapes=[pltpu.VMEM((head, head), F32)],
        cost_estimate=cost(1_000_000, 600_000),
        name="near_states",
        compiler_params=pltpu.CompilerParams(vmem_limit_bytes=2 << 20),
    )(states)
    states = pl.pallas_call(
        functools.partial(token_kernel, far_ranks),
        out_shape=shaped(states.shape, F32),
        in_specs=[VMEM] * 6 + [ANY],
        out_specs=ANY,
        scratch_shapes=[pltpu.VMEM((far, sequences, head), F32), pltpu.SemaphoreType.DMA],
        input_output_aliases={6: 0},
        cost_estimate=cost(20_000_000, 2_200_000),
        name="token",
        compiler_params=pltpu.CompilerParams(vmem_limit_bytes=6 << 20),
    )(token, later, w_query, w_forget, w_value, w_outgate, states)
    states = exchanged(states, HI, far_ranks)
    final, part = pl.pallas_call(
        functools.partial(far_kernel, far_ranks),
        out_shape=(shaped((rows, head), BF16), shaped((2 * near * far, head), F32)),
        in_specs=[VMEM] * 3,
        out_specs=(VMEM,) * 2,
        scratch_shapes=[pltpu.VMEM((head, head), F32)],
        cost_estimate=cost(1_000_000, 200_000),
        name="far_states",
        compiler_params=pltpu.CompilerParams(vmem_limit_bytes=2 << 20),
    )(states, gap, gain)
    part = exchanged(part.reshape(near * far, 1, 2 * head), SP, read_ranks).reshape(part.shape)
    first_read, cache = pl.pallas_call(
        read_kernel,
        out_shape=(shaped((sequences, head), BF16), shaped((rows, head), BF16)),
        in_specs=[VMEM] * 2,
        out_specs=(VMEM,) * 2,
        cost_estimate=cost(100_000, 40_000),
        name="read",
        compiler_params=pltpu.CompilerParams(vmem_limit_bytes=1 << 20),
    )(part, final)
    return cache[None], first_read


def solution(mesh):
    finer = Mesh(mesh.devices.reshape(8, 2, 4, mesh.shape["tp"]), (HI, LO, Y, TP))
    placed = (
        P(None, SP, None),
        P(None, SP),
        P(None, TP),
        P(None, TP),
        P(None, TP),
        P(None, TP),
        P(None, TP),
        P(TP),
        P(),
    )
    return jax.shard_map(
        device_step,
        mesh=finer,
        in_specs=placed,
        out_specs=(P(TP, SP, None), P(None, TP)),
        check_vma=False,
    )
```

```python
import functools

import jax
import jax.numpy as jnp
from jax import lax
from jax.experimental import pallas as pl
from jax.experimental.pallas import tpu as pltpu
from jax.sharding import Mesh
from jax.sharding import PartitionSpec as P


HI, LO, Y, TP = "sp_hi", "sp_lo", "sp_y", "tp"
SP = (HI, LO, Y)
NEAR = (LO, Y)
EPSILON = 1e-06
F32, BF16 = jnp.float32, jnp.bfloat16
FAR_ORDER = READ_ORDER = (4, 0, 7, 1, 6, 2, 5, 3)
NEAR_ORDER = (2, 0, 3, 1, 6, 4, 7, 5)


def read_order(near):
    return [h * len(near) + j for h in READ_ORDER for j in near]


def in_two(x):
    high = x.astype(BF16)
    return high, (x - high.astype(F32)).astype(BF16)


def opening_kernel(out_ref):
    out_ref[...] = jnp.zeros_like(out_ref)


def state_kernel(
    order, opening_ref, prompt_ref, keep_ref, gap_ref, wf_ref, wv_ref, out_ref, both_buf
):
    del opening_ref
    sequences, positions, width = prompt_ref.shape
    head = gap_ref.shape[1]
    peers = out_ref.shape[0]
    rows = head // peers
    pair = 2 * positions
    row = lax.broadcasted_iota(jnp.int32, (pair, pair), 0)
    column = lax.broadcasted_iota(jnp.int32, (pair, pair), 1)
    later_mask = (column > row) & (column // positions == row // positions)
    later_mask = later_mask.astype(F32).astype(BF16)
    filler = jnp.ones((sequences, head - positions), F32)
    keep_columns = jnp.transpose(jnp.concatenate([keep_ref[...], filler], axis=1))[:positions]
    log_columns = jnp.log(keep_columns)
    gap = gap_ref[...]

    def spread(columns, n):
        return jnp.concatenate(
            [
                jnp.broadcast_to(columns[:, s : s + 1], (positions, head))
                for s in (2 * n, 2 * n + 1)
            ],
            axis=0,
        )

    x = prompt_ref[...].reshape(sequences * positions, width)
    weights = jnp.concatenate([wf_ref[...], wv_ref[...]], axis=1)
    both_buf[...] = jnp.dot(x, weights, preferred_element_type=F32)
    for n in range(sequences // 2):
        both = both_buf[n * pair : (n + 1) * pair]
        values = both[:, head:].astype(BF16)
        loss = gap * jax.nn.sigmoid(-both[:, :head])
        keep_factor = spread(keep_columns, n)
        log_forget = spread(log_columns, n) + jnp.log1p(-loss)
        gate = (1.0 - keep_factor) + keep_factor * loss
        later = sum(
            jnp.dot(later_mask, part, preferred_element_type=F32)
            for part in in_two(log_forget)
        )
        gated = in_two(gate * jnp.exp(later))
        for k in range(2):
            s = 2 * n + k
            span = slice(k * positions, (k + 1) * positions)
            left = jnp.concatenate([part[span] for part in gated], axis=0)
            right = jnp.concatenate([values[span]] * 2, axis=0)
            state = lax.dot_general(
                left, right, (((0,), (0,)), ((), ())), preferred_element_type=F32
            )
            first = k * positions
            total = later[first : first + 1] + log_forget[first : first + 1]
            for r, j in enumerate(order):
                out_ref[r, s * rows : (s + 1) * rows, :] = state[j * rows : (j + 1) * rows]
                out_ref[r, head + s : head + s + 1, :] = total


def token_route(far, tp):
    return [(h * tp + (i ^ h ^ (tp - 1)), h * tp + i) for h in range(far) for i in range(tp)]


def near_kernel(
    order, far_ranks, in_ref, token_ref, wq_ref, wf_ref, wv_ref, wg_ref, out_ref, turned
):
    blocks = in_ref.shape[0]
    sequences, _, head = out_ref.shape
    rows = head // blocks
    width = token_ref.shape[1]
    block = lax.axis_index(TP) ^ lax.axis_index(HI) ^ (lax.axis_size(TP) - 1)
    span = pl.ds(pl.multiple_of(block * width, width), width)
    token = token_ref[...]
    parts = [
        jnp.dot(token, ref[span, :], preferred_element_type=F32)
        for ref in (wq_ref, wf_ref, wv_ref, wg_ref)
    ]
    later = jnp.zeros((sequences, head), F32)
    factors = [None] * blocks
    for b in reversed(range(blocks)):
        factors[b] = jnp.exp(later)
        later = later + in_ref[order.index(b), head : head + sequences, :]
    rest = jnp.zeros((head - blocks * sequences, head), F32)
    turned[...] = jnp.transpose(jnp.concatenate([*factors, rest], axis=0))
    mine = turned[pl.ds(pl.multiple_of(lax.axis_index(NEAR) * rows, rows), rows), :]
    spare = jnp.zeros((sequences - 1 - len(parts), head), F32)
    for s in range(sequences):
        total = jnp.zeros((rows, head), F32)
        for b in range(blocks):
            column = mine[:, b * sequences + s : b * sequences + s + 1]
            total = total + in_ref[order.index(b), s * rows : (s + 1) * rows, :] * column
        out_ref[far_ranks.index(s), :rows, :] = total
        out_ref[far_ranks.index(s), rows:, :] = jnp.concatenate(
            [later[s : s + 1], *(part[s : s + 1] for part in parts), spare], axis=0
        )


def far_kernel(order, in_ref, gap_ref, gain_ref, state_ref, part_ref, turned):
    blocks = in_ref.shape[0]
    rows, head = state_ref.shape
    later = jnp.zeros((1, head), F32)
    factors = [None] * blocks
    for b in reversed(range(blocks)):
        factors[b] = jnp.exp(later)
        later = later + in_ref[order.index(b), rows : rows + 1, :]
    tile = sum(in_ref[b, rows:, :] for b in range(blocks))
    query, forget, value, gate = (tile[k : k + 1] for k in range(1, 5))
    loss = gap_ref[...] * jax.nn.sigmoid(-forget)
    own = jnp.sum(query * loss, axis=1, keepdims=True) * value.astype(BF16).astype(F32)
    gate = gain_ref[...] * (gate * jax.nn.sigmoid(gate))
    weight = query * (1.0 - loss)
    rest = jnp.zeros((head - blocks - 1, head), F32)
    turned[...] = jnp.transpose(jnp.concatenate([*factors, weight, rest], axis=0))
    mine = turned[pl.ds(pl.multiple_of(lax.axis_index(NEAR) * rows, rows), rows), :]
    total = jnp.zeros((rows, head), F32)
    for b in range(blocks):
        total = total + in_ref[order.index(b), :rows, :] * mine[:, b : b + 1]
    state_ref[...] = total.astype(state_ref.dtype)
    part = jnp.sum(total * mine[:, blocks : blocks + 1], axis=0, keepdims=True)
    part = part + jnp.where(lax.axis_index(NEAR) == 0, own, 0.0)
    row = lax.broadcasted_iota(jnp.int32, part_ref.shape, 0)
    part_ref[...] = jnp.where(lax.rem(row, 2) == 0, part, gate)


def read_kernel(part_ref, state_ref, out_ref, cache_ref):
    cache_ref[...] = state_ref[...]
    sequences, head = out_ref.shape
    parts = part_ref[...].reshape(sequences, part_ref.shape[0] // sequences, head)
    row = lax.broadcasted_iota(jnp.int32, parts.shape, 1)
    mixed = jnp.sum(jnp.where(lax.rem(row, 2) == 0, parts, 0.0), axis=1)
    scale = lax.rsqrt(jnp.mean(mixed * mixed, axis=1, keepdims=True) + EPSILON)
    read = mixed * scale * parts[:, 1, :]
    places = [READ_ORDER.index(s) for s in range(sequences)]
    read = jnp.concatenate([read[a : a + 1] for a in places], axis=0)
    out_ref[...] = read.astype(out_ref.dtype)


def cost(flops, bytes_accessed):
    return pl.CostEstimate(flops=flops, bytes_accessed=bytes_accessed, transcendentals=0)


def exchanged(x, axes, ranks):
    return lax.all_to_all(x, axes, 0, 0, tiled=True, axis_index_groups=[ranks])


VMEM = pl.BlockSpec(memory_space=pltpu.VMEM)


def device_step(
    prompt, keep_scale, new_token, w_query, w_forget, w_value, w_outgate, floor_gap, norm_gain
):
    sequences, positions, _ = prompt.shape
    head = norm_gain.shape[0]
    near = lax.axis_size(NEAR)
    far = lax.axis_size(HI)
    rows = head // near
    near_ranks = list(NEAR_ORDER)
    far_ranks = list(FAR_ORDER)
    read_ranks = read_order(near_ranks)
    gap = floor_gap.reshape(1, head)
    gain = norm_gain.reshape(1, head)
    shaped = jax.ShapeDtypeStruct

    head_start = pl.pallas_call(
        opening_kernel,
        out_shape=shaped((8, head), F32),
        out_specs=VMEM,
        cost_estimate=cost(20_000_000_000, 40_000_000),
        name="opening",
        compiler_params=pltpu.CompilerParams(vmem_limit_bytes=1 << 20),
    )()
    token = lax.ppermute(new_token, (HI, TP), token_route(far, lax.axis_size(TP)))
    states = pl.pallas_call(
        functools.partial(state_kernel, near_ranks),
        out_shape=shaped((near, head + sequences, head), F32),
        in_specs=[VMEM] * 6,
        out_specs=VMEM,
        scratch_shapes=[pltpu.VMEM((sequences * positions, 2 * head), F32)],
        cost_estimate=cost(600_000_000, 4_000_000),
        name="block_states",
        compiler_params=pltpu.CompilerParams(vmem_limit_bytes=8 << 20),
    )(head_start, prompt, keep_scale, gap, w_forget, w_value)
    states, token = lax.optimization_barrier((states, token))
    states = exchanged(states, NEAR, near_ranks)
    states = pl.pallas_call(
        functools.partial(near_kernel, near_ranks, far_ranks),
        out_shape=shaped((far, rows + sequences, head), F32),
        in_specs=[VMEM] * 6,
        out_specs=VMEM,
        scratch_shapes=[pltpu.VMEM((head, head), F32)],
        cost_estimate=cost(20_000_000, 2_600_000),
        name="near_states",
        compiler_params=pltpu.CompilerParams(vmem_limit_bytes=6 << 20),
    )(states, token, w_query, w_forget, w_value, w_outgate)
    states = exchanged(states, HI, far_ranks)
    final, part = pl.pallas_call(
        functools.partial(far_kernel, far_ranks),
        out_shape=(shaped((rows, head), BF16), shaped((2 * near * far, head), F32)),
        in_specs=[VMEM] * 3,
        out_specs=(VMEM,) * 2,
        scratch_shapes=[pltpu.VMEM((head, head), F32)],
        cost_estimate=cost(1_000_000, 200_000),
        name="far_states",
        compiler_params=pltpu.CompilerParams(vmem_limit_bytes=2 << 20),
    )(states, gap, gain)
    part = exchanged(part.reshape(near * far, 1, 2 * head), SP, read_ranks).reshape(part.shape)
    first_read, cache = pl.pallas_call(
        read_kernel,
        out_shape=(shaped((sequences, head), BF16), shaped((rows, head), BF16)),
        in_specs=[VMEM] * 2,
        out_specs=(VMEM,) * 2,
        cost_estimate=cost(100_000, 40_000),
        name="read",
        compiler_params=pltpu.CompilerParams(vmem_limit_bytes=1 << 20),
    )(part, final)
    return cache[None], first_read


def solution(mesh):
    finer = Mesh(mesh.devices.reshape(8, 2, 4, mesh.shape["tp"]), (HI, LO, Y, TP))
    placed = (
        P(None, SP, None),
        P(None, SP),
        P(None, TP),
        P(None, TP),
        P(None, TP),
        P(None, TP),
        P(None, TP),
        P(TP),
        P(),
    )
    return jax.shard_map(
        device_step,
        mesh=finer,
        in_specs=placed,
        out_specs=(P(TP, SP, None), P(None, TP)),
        check_vma=False,
    )
```
